128 devices in a mesh: ep: 16 (over z, x), tp: 8 (over y, core).
Axes of the slice: x: 4, y: 4, z: 4, core: 2. Of those that a mesh axis runs over, the one named last changes fastest.
Arguments:
- tokens: bfloat16 [18432, 2048], P(('ep', 'tp')), may hold values from -6 to 6
- norm_gain: float32 [2048], replicated, may hold values from 0.1 to 1.9
- expert_ids: int32 [18432, 8], P(('ep', 'tp')), may hold values from 0 to 31, all different within a row; in each aligned block of 144 rows (0 to 143, 144 to 287, ...) at most 72 rows name the same one
- route_weights: float32 [18432, 8], P(('ep', 'tp')), may hold values from 0.3 to 1
- expert_gate: bfloat16 [32, 512, 2048], P('ep', 'tp'), may hold values from -0.125 to 0.125
- expert_up: bfloat16 [32, 512, 2048], P('ep', 'tp'), may hold values from -0.125 to 0.125
- expert_down: bfloat16 [32, 512, 2048], P('ep', 'tp'), may hold values from -0.25 to 0.25
- shared_gate: bfloat16 [512, 2048], P('tp'), may hold values from -0.125 to 0.125
- shared_up: bfloat16 [512, 2048], P('tp'), may hold values from -0.125 to 0.125
- shared_down: bfloat16 [512, 2048], P('tp'), may hold values from -0.25 to 0.25
- side_in: bfloat16 [2048, 1024], P('ep'), may hold values from -0.125 to 0.125
- side_out: bfloat16 [2048, 1024], P('ep'), may hold values from -0.1875 to 0.1875
- side_gate: bfloat16 [2048], replicated, may hold values from -0.125 to 0.125
Outputs:
- mixed: bfloat16 [18432, 2048], P(('ep', 'tp'))
The draws below stay inside these ranges and needn't reach their ends.
Inputs may be any that keep to these rules, and one draw needn't show every extreme that they name: `expert_ids`: each row names 8 different experts of 0 to 31; within the rows of one device (aligned blocks of 144 rows) no expert is named more than 72 times, and in some of those blocks some expert is named exactly 72 times.
All inputs are finite; a program needn't handle non-finite values.
Results may differ from the reference program's by a relative error of at most 0.0068.
Values may be sent and summed in bfloat16 or wider, within the bound.
A program may use at most 320 MiB of HBM per device.

```python
import math
import jax
import jax.numpy as jnp
import numpy as np
from jax import lax

D = 2048
FF = 512
SIDE = 1024
TOP = 8
TOK_DEV = 144
EXPERTS = 32
CAP = 72
TOKENS = 18432


def levels(stream_key, extent, pieces, smallest, largest):
    level = 1.0
    for dim, blocks in pieces:
        steps = jax.random.uniform(jax.random.fold_in(jax.random.fold_in(stream_key, 6), dim), (blocks,), jnp.float32, smallest / len(pieces), largest / len(pieces))
        level = level * jnp.repeat(jnp.exp(steps), extent[dim] // blocks).reshape((-1,) + (1,) * (len(extent) - 1 - dim))
    return level


def shared_out(rng, own, number, rows, number_of, top, bound, skew):
    ranking = jax.random.permutation(rng, number_of)
    heavy_load, common = portions_of(number_of, rows * top, bound, skew, True), portions_of(number_of, rows * top, bound, skew, False)
    places = jnp.arange(number_of)

    def named(lengths, rotation):
        used = int((lengths > 0).sum())
        fixed = max(1, used // 4)
        shifted = fixed + (places - fixed + rotation * (used - fixed)) % max(1, number_of - fixed)
        return jnp.zeros((number_of,), jnp.int32).at[ranking[jnp.where(places < fixed, places, shifted)]].set(jnp.asarray(lengths, jnp.int32))

    lengths = jnp.where(number % 4 == 0, named(heavy_load, number // 4), named(common, number - number // 4 - 1))
    mixed = jax.random.permutation(jax.random.fold_in(own, 3), number_of)
    source_of, receiver = mixed[0:number_of // 2 * 2:2], mixed[1:number_of // 2 * 2:2]
    slack = jnp.minimum(lengths[source_of] - 1, bound - lengths[receiver]) // 2
    slack = jnp.where((source_of == ranking[0]) | (receiver == ranking[0]) | (lengths[receiver] == 0), 0, jnp.maximum(slack, 0))
    shifted = jax.random.randint(jax.random.fold_in(own, 4), (number_of // 2,), 0, 1 << 20) % (slack + 1)
    lengths = lengths.at[source_of].add(-shifted).at[receiver].add(shifted)
    items = jnp.searchsorted(jnp.cumsum(lengths), jnp.arange(rows * top), side="right").astype(jnp.int32)
    listing = items.reshape(top, rows).T
    listing = listing[jax.random.permutation(jax.random.fold_in(own, 1), rows)]
    rotation = jax.random.randint(jax.random.fold_in(own, 2), (rows, 1), 0, top)
    return jnp.take_along_axis(listing, (jnp.arange(top)[None, :] + rotation) % top, axis=1)


def portions_of(amount, total, reach, slope, full):
    loads = [(1 << 20) // math.isqrt(rank ** slope) + 1 for rank in range(1, amount + 1)]
    largest = reach if full else min(reach, max(-(-total // amount), total * loads[0] // sum(loads)))
    least = 1 if total - largest >= amount - 1 else 0
    holding, spare = [largest] + [least] * (amount - 1), total - largest - least * (amount - 1)
    while spare > 0:
        free = [i for i in range(1, amount) if holding[i] < largest] or [i for i in range(1, amount) if holding[i] < reach]
        pool, left = sum([loads[i] for i in free]), spare
        for i in free:
            addition = min(reach - holding[i], max(1, left * loads[i] // pool), spare)
            holding[i] = holding[i] + addition
            spare = spare - addition
    return np.array(holding)


def centred(key, dims, scale, reach, split=(), kind=jnp.bfloat16):
    gain = levels(key, dims, split, -0.22, 0.18) if split else 1.0
    array = jax.random.normal(key, dims, jnp.float32) * scale * gain
    return jnp.minimum(jnp.maximum(array, -reach), reach).astype(kind)


def setup_inputs(seed: int = 0) -> dict:
    arg_keys = jax.random.split(jax.random.key(seed), 14)
    tokens = centred(arg_keys[0], (TOKENS, D), 1.0, 6.0, ((0, 128),))
    norm_gain = jnp.clip(1.0 + 0.18 * jax.random.normal(arg_keys[1], (D,), jnp.float32), 0.1, 1.9)
    expert_ids_keys = jax.random.split(jax.random.fold_in(arg_keys[2], 1), TOKENS // TOK_DEV)
    expert_ids_turns = jax.random.permutation(jax.random.fold_in(arg_keys[2], 3), TOKENS // TOK_DEV)
    expert_ids = jax.vmap(lambda own, number: shared_out(jax.random.fold_in(arg_keys[2], 2), own, number, TOK_DEV, EXPERTS, TOP, CAP, 2))(expert_ids_keys, expert_ids_turns).reshape((TOKENS, TOP))
    route_weights = jnp.clip(0.3 + 0.7 * jax.random.uniform(arg_keys[3], (TOKENS, TOP), jnp.float32) ** levels(arg_keys[3], (TOKENS, TOP), ((0, 128),), -0.2, 0.2), 0.3, 1.0)
    expert_gate = centred(arg_keys[4], (EXPERTS, FF, D), D ** -0.5, 0.125, ((0, 16), (1, 8)))
    expert_up = centred(arg_keys[5], (EXPERTS, FF, D), D ** -0.5, 0.125, ((0, 16), (1, 8)))
    expert_down = centred(arg_keys[6], (EXPERTS, FF, D), FF ** -0.5, 0.25, ((0, 16), (1, 8)))
    shared_gate = centred(arg_keys[7], (FF, D), D ** -0.5, 0.125, ((0, 8),))
    shared_up = centred(arg_keys[8], (FF, D), D ** -0.5, 0.125, ((0, 8),))
    shared_down = centred(arg_keys[9], (FF, D), FF ** -0.5, 0.25, ((0, 8),))
    side_in = centred(arg_keys[10], (D, SIDE), D ** -0.5, 0.125, ((0, 16),))
    side_out = centred(arg_keys[11], (D, SIDE), SIDE ** -0.5, 0.1875, ((0, 16),))
    side_gate = centred(arg_keys[12], (D,), D ** -0.5, 0.125)
    return dict(tokens=tokens, norm_gain=norm_gain, expert_ids=expert_ids, route_weights=route_weights, expert_gate=expert_gate, expert_up=expert_up, expert_down=expert_down, shared_gate=shared_gate, shared_up=shared_up, shared_down=shared_down, side_in=side_in, side_out=side_out, side_gate=side_gate)


norm_eps = 1.0
row_block = 512

def normalize(tokens, norm_gain):
    values = tokens.astype(jnp.float32)
    scale_inv = lax.rsqrt(lax.optimization_barrier(jnp.mean(values * values, axis=-1, keepdims=True)) + norm_eps)
    return (values * scale_inv * norm_gain).astype(jnp.bfloat16)

def swiglu(gate_part, up_part):
    return (jax.nn.silu(gate_part) * up_part).astype(jnp.bfloat16)

def reference(tokens, norm_gain, expert_ids, route_weights, expert_gate, expert_up, expert_down, shared_gate, shared_up, shared_down, side_in, side_out, side_gate):
    normed = normalize(tokens, norm_gain)
    pair_count = TOKENS * TOP
    flat_ids = expert_ids.reshape(pair_count).astype(jnp.int32)
    flat_tokens = (jnp.arange(pair_count, dtype=jnp.int32) // TOP).astype(jnp.int32)
    flat_weights = route_weights.reshape(pair_count)
    order = jnp.argsort(flat_ids, stable=True)
    sorted_ids = flat_ids[order]
    counts = jnp.bincount(flat_ids, length=EXPERTS).astype(jnp.int32)
    starts = (jnp.cumsum(counts) - counts).astype(jnp.int32)
    padded = ((counts + row_block - 1) // row_block * row_block).astype(jnp.int32)
    ends = jnp.cumsum(padded).astype(jnp.int32)
    begins = (ends - padded).astype(jnp.int32)
    target = (begins[sorted_ids] + jnp.arange(pair_count, dtype=jnp.int32) - starts[sorted_ids]).astype(jnp.int32)
    block_count = (pair_count + EXPERTS * (row_block - 1)) // row_block + 1
    slots_all = block_count * row_block
    token_slots = jnp.full((slots_all,), TOKENS, jnp.int32).at[target].set(flat_tokens[order])
    weight_slots = jnp.zeros((slots_all,), jnp.float32).at[target].set(flat_weights[order])
    block_starts = (jnp.arange(block_count, dtype=jnp.int32) * row_block).astype(jnp.int32)
    block_expert = jnp.minimum(jnp.searchsorted(ends, block_starts, side='right'), EXPERTS - 1).astype(jnp.int32)
    extended = jnp.concatenate([normed, jnp.zeros((1, D), normed.dtype)], axis=0)

    def block_step(running, inputs):
        slot_tokens, slot_weights, expert = inputs
        chosen = extended[slot_tokens]
        gate_part = jnp.dot(chosen, expert_gate[expert].T, preferred_element_type=jnp.float32)
        up_part = jnp.dot(chosen, expert_up[expert].T, preferred_element_type=jnp.float32)
        hidden = swiglu(gate_part, up_part)
        output = jnp.dot(hidden, expert_down[expert], preferred_element_type=jnp.float32).astype(jnp.bfloat16)
        output = lax.optimization_barrier(output).astype(jnp.float32)
        return (running.at[slot_tokens].add(output * slot_weights[:, None]), None)
    running = jnp.zeros((TOKENS + 1, D), jnp.float32)
    running, unused = lax.scan(block_step, running, (token_slots.reshape(block_count, row_block), weight_slots.reshape(block_count, row_block), block_expert))
    routed = running[:TOKENS]
    shared_hidden = swiglu(jnp.dot(normed, shared_gate.T, preferred_element_type=jnp.float32), jnp.dot(normed, shared_up.T, preferred_element_type=jnp.float32))
    shared = jnp.dot(shared_hidden, shared_down, preferred_element_type=jnp.float32)
    side_hidden = jax.nn.silu(jnp.dot(normed, side_in, preferred_element_type=jnp.float32)).astype(jnp.bfloat16)
    side_value = jnp.dot(side_hidden, side_out.T, preferred_element_type=jnp.float32)
    opening = jax.nn.sigmoid(jnp.dot(normed, side_gate, preferred_element_type=jnp.float32))
    return (routed + shared + opening[:, None] * side_value).astype(jnp.bfloat16)
```

```python
import functools

import jax
import jax.numpy as jnp
from jax import lax
from jax.experimental import pallas as pl
from jax.experimental.pallas import tpu as pltpu
from jax.sharding import PartitionSpec as P

norm_eps = 1.0
TOK = 144
D = 2048
HALF = 1024
SUB = 512
GROUP = 4
ROWS = GROUP * TOK

ORDER = [
    (2, 2), (2, 1), (2, 3), (2, 0),
    (1, 2), (1, 1), (3, 2), (3, 1),
    (1, 3), (1, 0), (3, 3), (3, 0),
    (0, 2), (0, 1), (0, 3), (0, 0),
]
SLOT = {place: i for i, place in enumerate(ORDER)}
DY = [0, 1, 3, 2]
DYI = {dy: i for i, dy in enumerate(DY)}
NT = (((1,), (1,)), ((), ()))


def kernel(
    tok_ref, gain_ref, w8_ref, gate_hbm, up_hbm, down_hbm, shared_hbm, side_hbm, sgate_ref,
    out_ref,
    xs, wg, wu, wd, wx, wdx, sb, sh, hid, rl, rf, rl2, rf2, wrow, wpat,
    ag_send, ag_m1, ag_f1, ag_m2, ag_f2,
    w_send, w_recv, w_fsend, w_frecv, w_dsend, w_drecv, w_loc,
    x_send, x_recv, x_loc, sb_dsend, sb_drecv, sh_send, sh_recv, sh_dsend, sh_drecv, sh_loc,
    rs_send, rl_sem, rf_sem, rl2_sem, rf2_sem,
):
    ep = lax.axis_index("ep")
    tp = lax.axis_index("tp")
    z, x = ep // 4, ep % 4
    y, core = tp // 2, tp % 2

    def at_ep(dz, dx):
        return (((z + dz) % 4) * 4 + (x + dx) % 4, tp)

    def at_y(dy):
        return (ep, ((y + dy) % 4) * 2 + core)

    partner = (ep, tp + 1 - 2 * core)

    def along(axis, step):
        return at_ep(step, 0) if axis == "z" else at_ep(0, step)

    def remote(src, dst, send, recv, where):
        return pltpu.make_async_remote_copy(
            src_ref=src, dst_ref=dst, send_sem=send, recv_sem=recv, device_id=where,
            device_id_type=pl.DeviceIdType.MESH,
        )

    wx[pl.ds(96, 32), :] = jnp.zeros((32, D), jnp.bfloat16)
    wx[pl.ds(128, 16), :] = sgate_ref[...]
    wx[pl.ds(144, 48), :] = jnp.zeros((48, D), jnp.bfloat16)
    wx[pl.ds(224, 32), :] = jnp.zeros((32, D), jnp.bfloat16)
    wdx[pl.ds(96, 32), :] = jnp.zeros((32, D), jnp.bfloat16)

    barrier = pltpu.get_barrier_semaphore()
    peers = [at_ep(*p) for p in ORDER if p != (0, 0)] + [at_y(d) for d in (1, 2, 3)] + [partner]
    for peer in peers:
        pl.semaphore_signal(barrier, inc=1, device_id=peer, device_id_type=pl.DeviceIdType.MESH)
    pl.semaphore_wait(barrier, len(peers))

    big = [(gate_hbm, wg), (up_hbm, wu), (down_hbm, wd)]
    w_p, w_m, w_fp, w_fm, w_d, w_l = [], [], [], [], {}, []
    for i, (src, dst) in enumerate(big):
        w_p.append(remote(src, dst.at[2 * DYI[3]], w_send.at[i, 0], w_recv.at[i, 0], at_y(1)))
        w_m.append(remote(src, dst.at[2 * DYI[1]], w_send.at[i, 1], w_recv.at[i, 1], at_y(3)))
        w_fp.append(remote(
            dst.at[2 * DYI[3], pl.ds(0, 64)], dst.at[2 * DYI[2], pl.ds(0, 64)],
            w_fsend.at[i, 0], w_frecv.at[i, 0], at_y(1)))
        w_fm.append(remote(
            dst.at[2 * DYI[1], pl.ds(64, 64)], dst.at[2 * DYI[2], pl.ds(64, 64)],
            w_fsend.at[i, 1], w_frecv.at[i, 1], at_y(3)))
        for dy in DY:
            w_d[i, dy] = remote(
                src if dy == 0 else dst.at[2 * DYI[dy]], dst.at[2 * DYI[dy] + 1],
                w_dsend.at[i, dy], w_drecv.at[i, dy], partner)
        w_l.append(pltpu.make_async_copy(src, dst.at[0], w_loc.at[i]))
    for i in range(3):
        w_p[i].start()
        w_m[i].start()
    for i in range(3):
        w_d[i, 0].start()
        w_l[i].start()

    values = tok_ref[...].astype(jnp.float32)
    scale_inv = lax.rsqrt(jnp.mean(values * values, axis=-1, keepdims=True) + norm_eps)
    normed = (values * scale_inv * gain_ref[...]).astype(jnp.bfloat16)
    xs[0, SLOT[0, 0]] = normed[:, :HALF]
    xs[1, SLOT[0, 0]] = normed[:, HALF:]

    axes = [("x", "z"), ("z", "x")]

    def src_slot(h, d1, d2):
        return SLOT[(d2, d1) if h == 0 else (d1, d2)]

    lo, hi = pl.ds(0, SUB), pl.ds(SUB, SUB)
    m1, f1, m2, f2 = {}, {}, {}, {}
    for h in range(2):
        a1, a2 = axes[h]
        s = functools.partial(src_slot, h)
        m1[h, 0] = remote(xs.at[h, s(0, 0)], xs.at[h, s(3, 0)], ag_send.at[h], ag_m1.at[h, 0], along(a1, 1))
        m1[h, 1] = remote(xs.at[h, s(0, 0)], xs.at[h, s(1, 0)], ag_send.at[h], ag_m1.at[h, 1], along(a1, 3))
        f1[h, 0] = remote(
            xs.at[h, s(3, 0), :, lo], xs.at[h, s(2, 0), :, lo], ag_send.at[h], ag_f1.at[h, 0], along(a1, 1))
        f1[h, 1] = remote(
            xs.at[h, s(1, 0), :, hi], xs.at[h, s(2, 0), :, hi], ag_send.at[h], ag_f1.at[h, 1], along(a1, 3))
        for d in range(4):
            m2[h, d, 0] = remote(
                xs.at[h, s(d, 0)], xs.at[h, s(d, 3)], ag_send.at[h], ag_m2.at[h, d, 0], along(a2, 1))
            m2[h, d, 1] = remote(
                xs.at[h, s(d, 0)], xs.at[h, s(d, 1)], ag_send.at[h], ag_m2.at[h, d, 1], along(a2, 3))
            f2[h, d, 0] = remote(
                xs.at[h, s(d, 3), :, lo], xs.at[h, s(d, 2), :, lo],
                ag_send.at[h], ag_f2.at[h, d, 0], along(a2, 1))
            f2[h, d, 1] = remote(
                xs.at[h, s(d, 1), :, hi], xs.at[h, s(d, 2), :, hi],
                ag_send.at[h], ag_f2.at[h, d, 1], along(a2, 3))

    both = [(h, k) for h in range(2) for k in range(2)]
    for h, k in both:
        m1[h, k].start()

    w_small, s_small = [], []
    for dz, dx in ORDER[:-1]:
        there = at_ep(dz, dx)
        mine = SLOT[(4 - dz) % 4, (4 - dx) % 4]
        w_small.append(remote(w8_ref.at[there[0]], wrow.at[mine], x_send.at[0], x_recv.at[0], there))
        s_small.append(remote(
            side_hbm.at[there[0]], sb.at[0, :, pl.ds(pl.multiple_of(ep * 128, 128), 128)],
            x_send.at[1], x_recv.at[1], there))
    for c in w_small + s_small:
        c.start()
    own_side = pltpu.make_async_copy(
        side_hbm.at[ep], sb.at[0, :, pl.ds(pl.multiple_of(ep * 128, 128), 128)], x_loc.at[0])
    own_side.start()
    wrow[SLOT[0, 0]] = w8_ref[ep]

    for h, k in both:
        m2[h, 0, k].start()

    owner = ep // 2
    is_src = tp == owner
    on_core = core == owner % 2
    sh_copies = [remote(shared_hbm, sh, sh_send.at[d - 1], sh_recv, at_y(d)) for d in (1, 2, 3)]
    sh_cross = remote(sh, sh, sh_dsend, sh_drecv, partner)
    sh_own = pltpu.make_async_copy(shared_hbm, sh, sh_loc)

    @pl.when(is_src)
    def _():
        for c in sh_copies:
            c.start()
        sh_own.start()
        sh_own.wait()
        sh_cross.start()

    for h, k in both:
        m1[h, k].wait_recv()
        f1[h, k].start()
    for h in range(2):
        for d in (3, 1):
            for k in range(2):
                m2[h, d, k].start()
    for h, k in both:
        m2[h, 0, k].wait_recv()
        f2[h, 0, k].start()

    pltpu.make_async_copy(wrow.at[pl.ds(0, 15)], wrow.at[pl.ds(0, 15)], x_recv.at[0]).wait()
    columns = jnp.transpose(wrow[...].reshape(128, 256))
    low_lane = lax.broadcasted_iota(jnp.int32, (TOK, 128), 1) < 64
    for i in range(16):
        wpat[i] = jnp.where(low_lane, columns[:TOK, 8 * i:8 * i + 1], columns[:TOK, 8 * i + 1:8 * i + 2])

    for h, k in both:
        f1[h, k].wait_recv()
    for h in range(2):
        for k in range(2):
            m2[h, 2, k].start()

    def weights_on(i):
        w_p[i].wait_recv()
        w_fp[i].start()
        w_d[i, 3].start()
        w_m[i].wait_recv()
        w_fm[i].start()
        w_d[i, 1].start()

    weights_on(0)
    own_side.wait()
    pltpu.make_async_copy(
        sb.at[0, :, pl.ds(0, 1920)], sb.at[0, :, pl.ds(0, 1920)], x_recv.at[1]).wait()
    sb_cross = remote(sb.at[0], sb.at[1], sb_dsend, sb_drecv, partner)
    sb_cross.start()
    for h, k in both:
        m2[h, 3, k].wait_recv()
        f2[h, 3, k].start()
    weights_on(1)
    for h, k in both:
        m2[h, 1, k].wait_recv()
        f2[h, 1, k].start()

    @pl.when(jnp.logical_and(on_core, jnp.logical_not(is_src)))
    def _():
        sh_copies[0].wait_recv()
        sh_cross.start()

    @pl.when(jnp.logical_not(on_core))
    def _():
        sh_cross.wait_recv()

    weights_on(2)
    for h, k in both:
        m2[h, 2, k].wait_recv()
        f2[h, 2, k].start()
    for i in range(3):
        w_fp[i].wait_recv()
        w_fm[i].wait_recv()
        w_d[i, 2].start()

    sb_cross.wait_recv()
    wx[pl.ds(0, 64), :] = sb[core]
    wdx[pl.ds(0, 64), :] = sb[1 - core]
    wx[pl.ds(64, 32), :] = sh[0]
    wx[pl.ds(192, 32), :] = sh[1]
    wdx[pl.ds(64, 32), :] = sh[2]

    for d in (0, 3, 1, 2):
        for h, k in both:
            f2[h, d, k].wait_recv()
    for i in range(3):
        w_l[i].wait()
        for dy in DY:
            w_d[i, dy].wait_recv()
    for h in range(2):
        pltpu.make_async_copy(xs.at[h, pl.ds(0, 15)], xs.at[h, pl.ds(0, 15)], ag_send.at[h]).wait()

    f32 = jnp.float32

    def silu(v):
        return v / (1.0 + jnp.exp(-v))

    def both_halves(xa, xb, w):
        return lax.dot_general(xa, w[:, :HALF], NT, preferred_element_type=f32) + lax.dot_general(
            xb, w[:, HALF:], NT, preferred_element_type=f32)

    def compute(group):
        base = GROUP * group
        pattern = wpat[pl.ds(base, GROUP)].reshape(ROWS, 128)

        def up_step(c, carry):
            xa = xs[0, pl.ds(base, GROUP)].reshape(ROWS, HALF)
            xb = xs[1, pl.ds(base, GROUP)].reshape(ROWS, HALF)
            rows = pl.ds(2 * c, 2)
            gate = both_halves(xa, xb, wg[rows].reshape(256, D))
            up = both_halves(xa, xb, wu[rows].reshape(256, D))
            w2 = jnp.concatenate([pattern, pattern], axis=1)
            hid[:, pl.ds(pl.multiple_of(c * 256, 256), 256)] = (silu(gate) * up * w2).astype(jnp.bfloat16)
            return carry

        lax.fori_loop(0, 4, up_step, 0)
        xa = xs[0, pl.ds(base, GROUP)].reshape(ROWS, HALF)
        xb = xs[1, pl.ds(base, GROUP)].reshape(ROWS, HALF)
        dense = both_halves(xa, xb, wx[...])
        first, second = dense[:, :128], dense[:, 128:]
        lane = lax.broadcasted_iota(jnp.int32, (ROWS, 128), 1)
        opening = 1.0 / (1.0 + jnp.exp(-second[:, :1]))
        factor = jnp.where(lane < 64, opening, second)
        hid[:, pl.ds(1024, 128)] = (silu(first) * factor).astype(jnp.bfloat16)

        def down_step(n, carry):
            h = n // 2
            cols = pl.ds(pl.multiple_of(n * SUB, SUB), SUB)
            to = pl.ds(pl.multiple_of((n % 2) * SUB, SUB), SUB)
            part = jnp.dot(hid[:, :1024], wd[:, :, cols].reshape(1024, SUB), preferred_element_type=f32)
            part = part + jnp.dot(hid[:, 1024:], wdx[:, cols], preferred_element_type=f32)
            xs[h, pl.ds(base, GROUP), :, to] = part.astype(jnp.bfloat16).reshape(GROUP, TOK, SUB)
            return carry

        lax.fori_loop(0, 4, down_step, 0)

    rs_axes = [("z", "x"), ("x", "z")]

    def dst_slot(h, d1, q):
        return SLOT[(d1, q) if h == 0 else (q, d1)]

    r1, s1, r2, s2 = {}, {}, {}, {}
    for h in range(2):
        b1, b2 = rs_axes[h]
        t = functools.partial(dst_slot, h)
        for q in range(4):
            r1[h, q, 0] = remote(
                xs.at[h, t(2, q), :, lo], rl.at[h, q, 0], rs_send.at[h], rl_sem.at[h, q, 0], along(b1, 1))
            r1[h, q, 1] = remote(
                xs.at[h, t(2, q), :, hi], rl.at[h, q, 1], rs_send.at[h], rl_sem.at[h, q, 1], along(b1, 3))
            s1[h, q, 0] = remote(
                xs.at[h, t(1, q)], rf.at[h, q, 0], rs_send.at[h], rf_sem.at[h, q, 0], along(b1, 1))
            s1[h, q, 1] = remote(
                xs.at[h, t(3, q)], rf.at[h, q, 1], rs_send.at[h], rf_sem.at[h, q, 1], along(b1, 3))
        r2[h, 0] = remote(
            xs.at[h, t(0, 2), :, lo], rl2.at[h, 0], rs_send.at[h], rl2_sem.at[h, 0], along(b2, 1))
        r2[h, 1] = remote(
            xs.at[h, t(0, 2), :, hi], rl2.at[h, 1], rs_send.at[h], rl2_sem.at[h, 1], along(b2, 3))
        s2[h, 0] = remote(xs.at[h, t(0, 1)], rf2.at[h, 0], rs_send.at[h], rf2_sem.at[h, 0], along(b2, 1))
        s2[h, 1] = remote(xs.at[h, t(0, 3)], rf2.at[h, 1], rs_send.at[h], rf2_sem.at[h, 1], along(b2, 3))

    def add(slot, h, cols, *more):
        total = xs[h, slot, :, cols].astype(f32)
        for m in more:
            total = total + m.astype(f32)
        xs[h, slot, :, cols] = total.astype(jnp.bfloat16)

    halves = [lo, hi]
    whole = pl.ds(0, HALF)

    def relay(h, q):
        for k in range(2):
            r1[h, q, k].start()

    def pass_on(h, q, k):
        r1[h, q, k].wait_recv()
        add(dst_slot(h, (1, 3)[k], q), h, halves[k], rl[h, q, k])
        s1[h, q, k].start()

    def collect(h, q):
        for k in range(2):
            s1[h, q, k].wait_recv()
        add(dst_slot(h, 0, q), h, whole, rf[h, q, 0], rf[h, q, 1])

    def relay2(h):
        for k in range(2):
            r2[h, k].start()

    def pass_on2(h, k):
        r2[h, k].wait_recv()
        add(dst_slot(h, 0, (1, 3)[k]), h, halves[k], rl2[h, k])
        s2[h, k].start()

    compute(0)
    relay(1, 2)
    for q in (2, 1, 3, 0):
        relay(0, q)
    compute(1)
    for q in (2, 1):
        pass_on(0, q, 0)
        pass_on(0, q, 1)
    for k in range(2):
        pass_on(1, 2, k)
    relay(1, 1)
    relay(1, 3)
    compute(2)
    for q in (3, 0):
        pass_on(0, q, 0)
        pass_on(0, q, 1)
    for q in (1, 3):
        for k in range(2):
            pass_on(1, q, k)
    collect(1, 2)
    relay2(1)
    compute(3)
    relay(1, 0)
    for q, k in ((1, 0), (3, 1)):
        collect(1, q)
        pass_on2(1, k)
    for k in range(2):
        pass_on(1, 0, k)
    collect(0, 2)
    relay2(0)
    for q, k in ((1, 0), (3, 1)):
        collect(0, q)
        pass_on2(0, k)
    collect(1, 0)
    collect(0, 0)
    for h in (1, 0):
        for k in range(2):
            s2[h, k].wait_recv()
        total = xs[h, SLOT[0, 0]].astype(f32) + rf2[h, 0].astype(f32) + rf2[h, 1].astype(f32)
        out_ref[:, pl.ds(h * HALF, HALF)] = total.astype(jnp.bfloat16)

    for h in range(2):
        pltpu.make_async_copy(xs.at[h, pl.ds(0, 15)], xs.at[h, pl.ds(0, 15)], rs_send.at[h]).wait()
    for i in range(3):
        w_p[i].wait_send()
        w_m[i].wait_send()
        w_fp[i].wait_send()
        w_fm[i].wait_send()
        for dy in DY:
            w_d[i, dy].wait_send()
    pltpu.make_async_copy(wrow.at[pl.ds(0, 15)], wrow.at[pl.ds(0, 15)], x_send.at[0]).wait()
    pltpu.make_async_copy(
        sb.at[0, :, pl.ds(0, 1920)], sb.at[0, :, pl.ds(0, 1920)], x_send.at[1]).wait()
    sb_cross.wait_send()

    @pl.when(is_src)
    def _():
        for c in sh_copies:
            c.wait_send()

    @pl.when(on_core)
    def _():
        sh_cross.wait_send()


def body(
    tokens, norm_gain, expert_ids, route_weights, expert_gate, expert_up, expert_down,
    shared_gate, shared_up, shared_down, side_in, side_out, side_gate,
):
    ep = lax.axis_index("ep")
    core = lax.axis_index("tp") % 2
    experts = jnp.arange(32, dtype=jnp.int32)
    chosen = expert_ids.T[None, :, :] == experts[:, None, None]
    dense = jnp.sum(jnp.where(chosen, route_weights.T[None, :, :], 0.0), axis=1)
    w8 = jnp.pad(dense.reshape(16, 2, TOK), ((0, 0), (0, 6), (0, 256 - TOK)))
    side = jnp.where(core == 0, side_in, side_out).T.reshape(16, 64, 128)
    first = (ep % 2) * 32
    shared = jnp.stack([
        lax.dynamic_slice_in_dim(a, first, 32, axis=0) for a in (shared_gate, shared_up, shared_down)
    ])
    sgate = jnp.pad(side_gate.reshape(1, D), ((0, 15), (0, 0)))
    bf16, f32 = jnp.bfloat16, jnp.float32
    dma, vmem = pltpu.SemaphoreType.DMA, pltpu.VMEM
    in_vmem = pl.BlockSpec(memory_space=pltpu.VMEM)
    in_any = pl.BlockSpec(memory_space=pl.ANY)
    return pl.pallas_call(
        kernel,
        out_shape=jax.ShapeDtypeStruct((TOK, D), bf16),
        in_specs=[in_vmem, in_vmem, in_vmem] + [in_any] * 5 + [in_vmem],
        out_specs=in_vmem,
        scratch_shapes=[
            vmem((2, 16, TOK, HALF), bf16),
            vmem((8, 128, D), bf16),
            vmem((8, 128, D), bf16),
            vmem((8, 128, D), bf16),
            vmem((256, D), bf16),
            vmem((128, D), bf16),
            vmem((2, 64, D), bf16),
            vmem((3, 32, D), bf16),
            vmem((ROWS, 1152), bf16),
            vmem((2, 4, 2, TOK, SUB), bf16),
            vmem((2, 4, 2, TOK, HALF), bf16),
            vmem((2, 2, TOK, SUB), bf16),
            vmem((2, 2, TOK, HALF), bf16),
            vmem((16, 8, 256), f32),
            vmem((16, TOK, 128), f32),
            dma((2,)), dma((2, 2)), dma((2, 2)), dma((2, 4, 2)), dma((2, 4, 2)),
            dma((3, 2)), dma((3, 2)), dma((3, 2)), dma((3, 2)), dma((3, 4)), dma((3, 4)), dma((3,)),
            dma((2,)), dma((2,)), dma((1,)), dma(()), dma(()), dma((3,)), dma(()), dma(()), dma(()), dma(()),
            dma((2,)), dma((2, 4, 2)), dma((2, 4, 2)), dma((2, 2)), dma((2, 2)),
        ],
        compiler_params=pltpu.CompilerParams(
            collective_id=0, has_side_effects=True, vmem_limit_bytes=60 * 1024 * 1024),
        name="routed_layer",
    )(
        tokens, norm_gain.reshape(1, D), w8,
        expert_gate.reshape(128, D), expert_up.reshape(128, D), expert_down.reshape(128, D),
        shared, side, sgate,
    )


def solution(mesh):
    placed = (
        P(("ep", "tp"), None),
        P(),
        P(("ep", "tp"), None),
        P(("ep", "tp"), None),
        P("ep", "tp", None),
        P("ep", "tp", None),
        P("ep", "tp", None),
        P("tp", None),
        P("tp", None),
        P("tp", None),
        P("ep", None),
        P("ep", None),
        P(),
    )
    return jax.shard_map(
        body, mesh=mesh, in_specs=placed, out_specs=P(("ep", "tp"), None), check_vma=False
    )
```

```python
import functools

import jax
import jax.numpy as jnp
from jax import lax
from jax.experimental import pallas as pl
from jax.experimental.pallas import tpu as pltpu
from jax.sharding import PartitionSpec as P

norm_eps = 1.0
TOK = 144
D = 2048
HALF = 1024
SUB = 512
GROUP = 4
ROWS = GROUP * TOK

ORDER = [
    (2, 2), (1, 2), (2, 1), (2, 3),
    (3, 3), (3, 2), (0, 2), (2, 0),
    (1, 1), (1, 3), (3, 1), (3, 0),
    (1, 0), (0, 1), (0, 3), (0, 0),
]
GROUPS = [12, 8, 4, 0]
PAIRS = {
    "g3a": 0, "g3b": 2, "g2a": 4, "g2b": 6, "g1a": 8, "g1b": 10, "g0a": 12, "g0b": 14,
}
SUM_ORDER = [
    ("C", "gu3a"), ("C", "g2b"), ("relay", 1, 0, 1), ("relay", 1, 0, 0), ("relay", 0, 0, 0), ("relay", 0, 0, 1),
    ("C", "g1a"), ("free", 0, 3, 0), ("free", 1, 1, 0), ("free", 0, 1, 0), ("free", 1, 1, 1), ("C", "g2a"),
    ("relay", 1, 3, 0), ("relay", 1, 3, 1), ("free", 0, 2, 1), ("free", 0, 3, 1), ("free", 1, 3, 1), ("C", "gu3b"),
    ("C", "g3a"), ("relay", 1, 2, 0), ("relay", 0, 2, 1), ("relay", 0, 2, 0), ("relay", 1, 2, 1), ("relay", 1, 1, 1),
    ("free", 0, 2, 0), ("relay", 1, 1, 0), ("C", "g3b"), ("relay", 0, 3, 1), ("relay", 0, 3, 0), ("free", 1, 2, 1),
    ("free", 1, 2, 0), ("relay", 0, 1, 1), ("relay", 0, 1, 0), ("C", "g0a"), ("pass", 1, 3, 1), ("free", 1, 0, 0),
    ("pass", 0, 0, 0), ("pass", 1, 0, 0), ("free", 0, 0, 0), ("C", "g1b"), ("free", 1, 3, 0), ("pass", 1, 2, 0),
    ("pass", 0, 2, 1), ("pass", 0, 2, 0), ("pass", 1, 3, 0), ("free", 0, 1, 1), ("free", 0, 0, 1), ("pass", 0, 0, 1),
    ("C", "g0b"), ("pass", 1, 2, 1), ("pass", 0, 3, 1), ("free", 1, 0, 1), ("pass", 1, 1, 0), ("pass", 1, 0, 1),
    ("pass", 0, 3, 0), ("pass", 1, 1, 1), ("pass", 0, 1, 1), ("pass", 0, 1, 0), ("collect", 0, 2, 0),
    ("relay2", 0, 0, 0), ("relay2", 0, 0, 1), ("collect", 1, 2, 0), ("relay2", 1, 0, 0), ("relay2", 1, 0, 1),
    ("collect", 0, 0, 0), ("collect", 1, 3, 0), ("free2", 1, 0, 1), ("collect", 0, 3, 0), ("free2", 0, 0, 1),
    ("collect", 1, 0, 0), ("collect", 1, 1, 0), ("free2", 1, 0, 0), ("collect", 0, 1, 0), ("free2", 0, 0, 0),
    ("pass2", 0, 0, 0), ("pass2", 0, 0, 1), ("pass2", 1, 0, 0), ("pass2", 1, 0, 1), ("final", 0, 0, 0),
    ("final", 1, 0, 0),
]
SLOT = {place: i for i, place in enumerate(ORDER)}
DY = [0, 1, 3, 2]
DYI = {dy: i for i, dy in enumerate(DY)}
NT = (((1,), (1,)), ((), ()))


def kernel(
    tok_ref, gain_ref, w8_ref, gate_hbm, up_hbm, down_hbm, shared_hbm, side_hbm, sgate_ref,
    out_ref,
    xs, wg, wu, wd, wx, wdx, sb, sh, hid, rl, rf, rl2, rf2, wrow, wpat,
    ag_send, ag_m1, ag_f1, ag_m2, ag_f2,
    w_send, w_recv, w_fsend, w_frecv, w_dsend, w_drecv, w_loc,
    x_send, x_recv, x_loc, sb_dsend, sb_drecv, sh_send, sh_recv, sh_dsend, sh_drecv, sh_loc,
    rs_send, rl_sem, rf_sem, rl2_sem, rf2_sem,
):
    ep = lax.axis_index("ep")
    tp = lax.axis_index("tp")
    z, x = ep // 4, ep % 4
    y, core = tp // 2, tp % 2

    def at_ep(dz, dx):
        return (((z + dz) % 4) * 4 + (x + dx) % 4, tp)

    def at_y(dy):
        return (ep, ((y + dy) % 4) * 2 + core)

    partner = (ep, tp + 1 - 2 * core)

    def along(axis, step):
        return at_ep(step, 0) if axis == "z" else at_ep(0, step)

    def remote(src, dst, send, recv, where):
        return pltpu.make_async_remote_copy(
            src_ref=src, dst_ref=dst, send_sem=send, recv_sem=recv, device_id=where,
            device_id_type=pl.DeviceIdType.MESH,
        )

    wx[pl.ds(96, 32), :] = jnp.zeros((32, D), jnp.bfloat16)
    wx[pl.ds(128, 16), :] = sgate_ref[...]
    wx[pl.ds(144, 48), :] = jnp.zeros((48, D), jnp.bfloat16)
    wx[pl.ds(224, 32), :] = jnp.zeros((32, D), jnp.bfloat16)
    wdx[pl.ds(96, 32), :] = jnp.zeros((32, D), jnp.bfloat16)

    barrier = pltpu.get_barrier_semaphore()
    peers = [at_ep(*p) for p in ORDER if p != (0, 0)] + [at_y(d) for d in (1, 2, 3)] + [partner]
    for peer in peers:
        pl.semaphore_signal(barrier, inc=1, device_id=peer, device_id_type=pl.DeviceIdType.MESH)
    pl.semaphore_wait(barrier, len(peers))

    big = [(gate_hbm, wg), (up_hbm, wu), (down_hbm, wd)]
    w_p, w_m, w_fp, w_fm, w_d, w_l = [], [], [], [], {}, []
    for i, (src, dst) in enumerate(big):
        w_p.append(remote(src, dst.at[2 * DYI[3]], w_send.at[i, 0], w_recv.at[i, 0], at_y(1)))
        w_m.append(remote(src, dst.at[2 * DYI[1]], w_send.at[i, 1], w_recv.at[i, 1], at_y(3)))
        w_fp.append(remote(
            dst.at[2 * DYI[3], pl.ds(0, 64)], dst.at[2 * DYI[2], pl.ds(0, 64)],
            w_fsend.at[i, 0], w_frecv.at[i, 0], at_y(1)))
        w_fm.append(remote(
            dst.at[2 * DYI[1], pl.ds(64, 64)], dst.at[2 * DYI[2], pl.ds(64, 64)],
            w_fsend.at[i, 1], w_frecv.at[i, 1], at_y(3)))
        for dy in DY:
            w_d[i, dy] = remote(
                src if dy == 0 else dst.at[2 * DYI[dy]], dst.at[2 * DYI[dy] + 1],
                w_dsend.at[i, dy], w_drecv.at[i, dy], partner)
        w_l.append(pltpu.make_async_copy(src, dst.at[0], w_loc.at[i]))
    for i in range(2):
        w_p[i].start()
        w_m[i].start()
    for i in range(3):
        w_d[i, 0].start()
        w_l[i].start()

    values = tok_ref[...].astype(jnp.float32)
    scale_inv = lax.rsqrt(jnp.mean(values * values, axis=-1, keepdims=True) + norm_eps)
    normed = (values * scale_inv * gain_ref[...]).astype(jnp.bfloat16)
    xs[0, SLOT[0, 0]] = normed[:, :HALF]
    xs[1, SLOT[0, 0]] = normed[:, HALF:]

    axes = [("x", "z"), ("z", "x")]

    def src_slot(h, d1, d2):
        return SLOT[(d2, d1) if h == 0 else (d1, d2)]

    lo, hi = pl.ds(0, SUB), pl.ds(SUB, SUB)
    m1, f1, m2, f2 = {}, {}, {}, {}
    for h in range(2):
        a1, a2 = axes[h]
        s = functools.partial(src_slot, h)
        m1[h, 0] = remote(xs.at[h, s(0, 0)], xs.at[h, s(3, 0)], ag_send.at[h], ag_m1.at[h, 0], along(a1, 1))
        m1[h, 1] = remote(xs.at[h, s(0, 0)], xs.at[h, s(1, 0)], ag_send.at[h], ag_m1.at[h, 1], along(a1, 3))
        f1[h, 0] = remote(
            xs.at[h, s(3, 0), :, lo], xs.at[h, s(2, 0), :, lo], ag_send.at[h], ag_f1.at[h, 0], along(a1, 1))
        f1[h, 1] = remote(
            xs.at[h, s(1, 0), :, hi], xs.at[h, s(2, 0), :, hi], ag_send.at[h], ag_f1.at[h, 1], along(a1, 3))
        for d in range(4):
            m2[h, d, 0] = remote(
                xs.at[h, s(d, 0)], xs.at[h, s(d, 3)], ag_send.at[h], ag_m2.at[h, d, 0], along(a2, 1))
            m2[h, d, 1] = remote(
                xs.at[h, s(d, 0)], xs.at[h, s(d, 1)], ag_send.at[h], ag_m2.at[h, d, 1], along(a2, 3))
            f2[h, d, 0] = remote(
                xs.at[h, s(d, 3), :, lo], xs.at[h, s(d, 2), :, lo],
                ag_send.at[h], ag_f2.at[h, d, 0], along(a2, 1))
            f2[h, d, 1] = remote(
                xs.at[h, s(d, 1), :, hi], xs.at[h, s(d, 2), :, hi],
                ag_send.at[h], ag_f2.at[h, d, 1], along(a2, 3))

    both = [(h, k) for h in range(2) for k in range(2)]
    for h, k in both:
        m1[h, k].start()

    w_small, s_small = [], []
    for dz, dx in ORDER[:-1]:
        there = at_ep(dz, dx)
        mine = SLOT[(4 - dz) % 4, (4 - dx) % 4]
        w_small.append(remote(w8_ref.at[there[0]], wrow.at[mine], x_send.at[0], x_recv.at[0], there))
        s_small.append(remote(
            side_hbm.at[there[0]], sb.at[0, :, pl.ds(pl.multiple_of(ep * 128, 128), 128)],
            x_send.at[1], x_recv.at[1], there))
    for c in w_small + s_small:
        c.start()
    own_side = pltpu.make_async_copy(
        side_hbm.at[ep], sb.at[0, :, pl.ds(pl.multiple_of(ep * 128, 128), 128)], x_loc.at[0])
    own_side.start()
    wrow[SLOT[0, 0]] = w8_ref[ep]

    for h, k in both:
        m2[h, 0, k].start()

    owner = ep // 2
    is_src = tp == owner
    on_core = core == owner % 2
    sh_copies = [remote(shared_hbm, sh, sh_send.at[d - 1], sh_recv, at_y(d)) for d in (1, 2, 3)]
    sh_cross = remote(sh, sh, sh_dsend, sh_drecv, partner)
    sh_own = pltpu.make_async_copy(shared_hbm, sh, sh_loc)

    @pl.when(is_src)
    def _():
        for c in sh_copies:
            c.start()
        sh_own.start()
        sh_own.wait()
        sh_cross.start()

    f32 = jnp.float32

    def silu(v):
        return v / (1.0 + jnp.exp(-v))

    def both_halves(xa, xb, w):
        return lax.dot_general(xa, w[:, :HALF], NT, preferred_element_type=f32) + lax.dot_general(
            xb, w[:, HALF:], NT, preferred_element_type=f32)

    def rows_of(base):
        return (xs[0, pl.ds(base, GROUP)].reshape(ROWS, HALF), xs[1, pl.ds(base, GROUP)].reshape(ROWS, HALF))

    def hidden(base, first, count):
        pattern = wpat[pl.ds(base, GROUP)].reshape(ROWS, 128)
        w2 = jnp.concatenate([pattern, pattern], axis=1)

        def step(c, carry):
            xa, xb = rows_of(base)
            rows = pl.ds(2 * c, 2)
            gate = both_halves(xa, xb, wg[rows].reshape(256, D))
            up = both_halves(xa, xb, wu[rows].reshape(256, D))
            value = (silu(gate) * up * w2).astype(jnp.bfloat16)
            hid[pl.ds(base, GROUP), :, pl.ds(pl.multiple_of(c * 256, 256), 256)] = value.reshape(GROUP, TOK, 256)
            return carry

        lax.fori_loop(first, first + count, step, 0)

    def dense_hidden(base):
        xa, xb = rows_of(base)
        dense = both_halves(xa, xb, wx[...])
        first, second = dense[:, :128], dense[:, 128:]
        lane = lax.broadcasted_iota(jnp.int32, (ROWS, 128), 1)
        opening = 1.0 / (1.0 + jnp.exp(-second[:, :1]))
        factor = jnp.where(lane < 64, opening, second)
        value = (silu(first) * factor).astype(jnp.bfloat16)
        hid[pl.ds(base, GROUP), :, pl.ds(1024, 128)] = value.reshape(GROUP, TOK, 128)

    def down(base):
        def step(n, carry):
            h = n // 2
            cols = pl.ds(pl.multiple_of(n * SUB, SUB), SUB)
            to = pl.ds(pl.multiple_of((n % 2) * SUB, SUB), SUB)
            rows = hid[pl.ds(base, 2)].reshape(2 * TOK, 1152)
            part = jnp.dot(rows[:, :1024], wd[:, :, cols].reshape(1024, SUB), preferred_element_type=f32)
            part = part + jnp.dot(rows[:, 1024:], wdx[:, cols], preferred_element_type=f32)
            xs[h, pl.ds(base, 2), :, to] = part.astype(jnp.bfloat16).reshape(2, TOK, SUB)
            return carry

        lax.fori_loop(0, 4, step, 0)

    for h, k in both:
        m1[h, k].wait_recv()
        f1[h, k].start()
    for h in range(2):
        for d in (3, 1):
            for k in range(2):
                m2[h, d, k].start()

    def weights_on(i):
        w_p[i].wait_recv()
        w_fp[i].start()
        w_d[i, 3].start()
        w_m[i].wait_recv()
        w_fm[i].start()
        w_d[i, 1].start()

    def weights_far(i):
        w_fp[i].wait_recv()
        w_fm[i].wait_recv()
        w_d[i, 2].start()

    weights_on(0)

    pltpu.make_async_copy(wrow.at[pl.ds(0, 15)], wrow.at[pl.ds(0, 15)], x_recv.at[0]).wait()
    columns = jnp.transpose(wrow[...].reshape(128, 256))
    low_lane = lax.broadcasted_iota(jnp.int32, (TOK, 128), 1) < 64
    for i in range(16):
        wpat[i] = jnp.where(low_lane, columns[:TOK, 8 * i:8 * i + 1], columns[:TOK, 8 * i + 1:8 * i + 2])

    for h, k in both:
        m2[h, 0, k].wait_recv()
        f2[h, 0, k].start()
    for i in range(2):
        w_l[i].wait()
        w_d[i, 0].wait_recv()
    hidden(GROUPS[0], 0, 1)
    for h, k in both:
        f1[h, k].wait_recv()
    for h in range(2):
        for k in range(2):
            m2[h, 2, k].start()
    own_side.wait()
    pltpu.make_async_copy(
        sb.at[0, :, pl.ds(0, 1920)], sb.at[0, :, pl.ds(0, 1920)], x_recv.at[1]).wait()
    sb_cross = remote(sb.at[0], sb.at[1], sb_dsend, sb_drecv, partner)
    sb_cross.start()
    weights_on(1)
    w_p[2].start()
    w_m[2].start()
    for h, k in both:
        m2[h, 3, k].wait_recv()
        f2[h, 3, k].start()
    for i in range(2):
        w_d[i, 1].wait_recv()
        w_d[i, 3].wait_recv()
    hidden(GROUPS[0], 1, 2)

    @pl.when(jnp.logical_and(on_core, jnp.logical_not(is_src)))
    def _():
        sh_copies[0].wait_recv()
        sh_cross.start()

    @pl.when(jnp.logical_not(on_core))
    def _():
        sh_cross.wait_recv()

    sb_cross.wait_recv()
    wx[pl.ds(0, 64), :] = sb[core]
    wdx[pl.ds(0, 64), :] = sb[1 - core]
    wx[pl.ds(64, 32), :] = sh[0]
    wx[pl.ds(192, 32), :] = sh[1]
    wdx[pl.ds(64, 32), :] = sh[2]
    dense_hidden(GROUPS[0])
    for h, k in both:
        m2[h, 1, k].wait_recv()
        f2[h, 1, k].start()
    weights_far(0)
    hidden(GROUPS[1], 0, 3)
    weights_far(1)
    for h, k in both:
        f2[h, 0, k].wait_recv()
    for i in range(2):
        w_d[i, 2].wait_recv()
    hidden(GROUPS[0], 3, 1)
    hidden(GROUPS[1], 3, 1)
    for h, k in both:
        m2[h, 2, k].wait_recv()
        f2[h, 2, k].start()
    for h, k in both:
        f2[h, 3, k].wait_recv()
    hidden(GROUPS[2], 0, 2)
    weights_on(2)
    hidden(GROUPS[2], 2, 2)
    dense_hidden(GROUPS[1])
    dense_hidden(GROUPS[2])
    for d in (1, 2):
        for h, k in both:
            f2[h, d, k].wait_recv()
    for h in range(2):
        pltpu.make_async_copy(xs.at[h, pl.ds(0, 15)], xs.at[h, pl.ds(0, 15)], ag_send.at[h]).wait()

    def last_hidden(part):
        if part == "gu3a":
            hidden(GROUPS[3], 0, 1)
            weights_far(2)
            hidden(GROUPS[3], 1, 1)
            w_l[2].wait()
            for dy in DY:
                w_d[2, dy].wait_recv()
        else:
            hidden(GROUPS[3], 2, 2)
            dense_hidden(GROUPS[3])

    rs_axes = [("z", "x"), ("x", "z")]

    def dst_slot(h, d1, q):
        return SLOT[(d1, q) if h == 0 else (q, d1)]

    r1, s1, e1, r2, s2, e2 = {}, {}, {}, {}, {}, {}
    halves = [lo, hi]
    for h in range(2):
        b1, b2 = rs_axes[h]
        t = functools.partial(dst_slot, h)
        for k in range(2):
            sum_cols, own_cols = halves[k], halves[1 - k]
            near, step = (1, 3)[k], (1, 3)[k]
            for q in range(4):
                to = along(b1, step)
                r1[h, q, k] = remote(
                    xs.at[h, t(2, q), :, sum_cols], rl.at[h, q, k], rs_send.at[h], rl_sem.at[h, q, k], to)
                s1[h, q, k] = remote(
                    xs.at[h, t(near, q), :, sum_cols], rf.at[h, q, k, :, sum_cols],
                    rs_send.at[h], rf_sem.at[h, q, k, 0], to)
                e1[h, q, k] = remote(
                    xs.at[h, t(near, q), :, own_cols], rf.at[h, q, k, :, own_cols],
                    rs_send.at[h], rf_sem.at[h, q, k, 1], to)
            to = along(b2, step)
            r2[h, k] = remote(
                xs.at[h, t(0, 2), :, sum_cols], rl2.at[h, k], rs_send.at[h], rl2_sem.at[h, k], to)
            s2[h, k] = remote(
                xs.at[h, t(0, near), :, sum_cols], rf2.at[h, k, :, sum_cols],
                rs_send.at[h], rf2_sem.at[h, k, 0], to)
            e2[h, k] = remote(
                xs.at[h, t(0, near), :, own_cols], rf2.at[h, k, :, own_cols],
                rs_send.at[h], rf2_sem.at[h, k, 1], to)

    def add(slot, h, cols, *more):
        total = xs[h, slot, :, cols].astype(f32)
        for m in more:
            total = total + m.astype(f32)
        xs[h, slot, :, cols] = total.astype(jnp.bfloat16)

    for op in SUM_ORDER:
        name = op[0]
        if name == "C":
            if op[1] in PAIRS:
                down(PAIRS[op[1]])
            else:
                last_hidden(op[1])
            continue
        _, h, q, k = op
        near = (1, 3)[k]
        if name == "relay":
            r1[h, q, k].start()
        elif name == "free":
            e1[h, q, k].start()
        elif name == "pass":
            r1[h, q, k].wait_recv()
            add(dst_slot(h, near, q), h, halves[k], rl[h, q, k])
            s1[h, q, k].start()
        elif name == "collect":
            for i in range(2):
                e1[h, q, i].wait_recv()
                s1[h, q, i].wait_recv()
            add(dst_slot(h, 0, q), h, pl.ds(0, HALF), rf[h, q, 0], rf[h, q, 1])
        elif name == "relay2":
            r2[h, k].start()
        elif name == "free2":
            e2[h, k].start()
        elif name == "pass2":
            r2[h, k].wait_recv()
            add(dst_slot(h, 0, near), h, halves[k], rl2[h, k])
            s2[h, k].start()
        else:
            for i in range(2):
                e2[h, i].wait_recv()
                s2[h, i].wait_recv()
            total = xs[h, SLOT[0, 0]].astype(f32) + rf2[h, 0].astype(f32) + rf2[h, 1].astype(f32)
            out_ref[:, pl.ds(h * HALF, HALF)] = total.astype(jnp.bfloat16)

    for h in range(2):
        pltpu.make_async_copy(xs.at[h, pl.ds(0, 15)], xs.at[h, pl.ds(0, 15)], rs_send.at[h]).wait()
    for i in range(3):
        w_p[i].wait_send()
        w_m[i].wait_send()
        w_fp[i].wait_send()
        w_fm[i].wait_send()
        for dy in DY:
            w_d[i, dy].wait_send()
    pltpu.make_async_copy(wrow.at[pl.ds(0, 15)], wrow.at[pl.ds(0, 15)], x_send.at[0]).wait()
    pltpu.make_async_copy(
        sb.at[0, :, pl.ds(0, 1920)], sb.at[0, :, pl.ds(0, 1920)], x_send.at[1]).wait()
    sb_cross.wait_send()

    @pl.when(is_src)
    def _():
        for c in sh_copies:
            c.wait_send()

    @pl.when(on_core)
    def _():
        sh_cross.wait_send()


def body(
    tokens, norm_gain, expert_ids, route_weights, expert_gate, expert_up, expert_down,
    shared_gate, shared_up, shared_down, side_in, side_out, side_gate,
):
    ep = lax.axis_index("ep")
    core = lax.axis_index("tp") % 2
    experts = jnp.arange(32, dtype=jnp.int32)
    chosen = expert_ids.T[None, :, :] == experts[:, None, None]
    dense = jnp.sum(jnp.where(chosen, route_weights.T[None, :, :], 0.0), axis=1)
    w8 = jnp.pad(dense.reshape(16, 2, TOK), ((0, 0), (0, 6), (0, 256 - TOK)))
    side = jnp.where(core == 0, side_in, side_out).T.reshape(16, 64, 128)
    first = (ep % 2) * 32
    shared = jnp.stack([
        lax.dynamic_slice_in_dim(a, first, 32, axis=0) for a in (shared_gate, shared_up, shared_down)
    ])
    sgate = jnp.pad(side_gate.reshape(1, D), ((0, 15), (0, 0)))
    bf16, f32 = jnp.bfloat16, jnp.float32
    dma, vmem = pltpu.SemaphoreType.DMA, pltpu.VMEM
    in_vmem = pl.BlockSpec(memory_space=pltpu.VMEM)
    in_any = pl.BlockSpec(memory_space=pl.ANY)
    return pl.pallas_call(
        kernel,
        out_shape=jax.ShapeDtypeStruct((TOK, D), bf16),
        in_specs=[in_vmem, in_vmem, in_vmem] + [in_any] * 5 + [in_vmem],
        out_specs=in_vmem,
        scratch_shapes=[
            vmem((2, 16, TOK, HALF), bf16),
            vmem((8, 128, D), bf16),
            vmem((8, 128, D), bf16),
            vmem((8, 128, D), bf16),
            vmem((256, D), bf16),
            vmem((128, D), bf16),
            vmem((2, 64, D), bf16),
            vmem((3, 32, D), bf16),
            vmem((16, TOK, 1152), bf16),
            vmem((2, 4, 2, TOK, SUB), bf16),
            vmem((2, 4, 2, TOK, HALF), bf16),
            vmem((2, 2, TOK, SUB), bf16),
            vmem((2, 2, TOK, HALF), bf16),
            vmem((16, 8, 256), f32),
            vmem((16, TOK, 128), f32),
            dma((2,)), dma((2, 2)), dma((2, 2)), dma((2, 4, 2)), dma((2, 4, 2)),
            dma((3, 2)), dma((3, 2)), dma((3, 2)), dma((3, 2)), dma((3, 4)), dma((3, 4)), dma((3,)),
            dma((2,)), dma((2,)), dma((1,)), dma(()), dma(()), dma((3,)), dma(()), dma(()), dma(()), dma(()),
            dma((2,)), dma((2, 4, 2)), dma((2, 4, 2, 2)), dma((2, 2)), dma((2, 2, 2)),
        ],
        compiler_params=pltpu.CompilerParams(
            collective_id=0, has_side_effects=True, vmem_limit_bytes=60 * 1024 * 1024),
        name="routed_layer",
    )(
        tokens, norm_gain.reshape(1, D), w8,
        expert_gate.reshape(128, D), expert_up.reshape(128, D), expert_down.reshape(128, D),
        shared, side, sgate,
    )


def solution(mesh):
    placed = (
        P(("ep", "tp"), None),
        P(),
        P(("ep", "tp"), None),
        P(("ep", "tp"), None),
        P("ep", "tp", None),
        P("ep", "tp", None),
        P("ep", "tp", None),
        P("tp", None),
        P("tp", None),
        P("tp", None),
        P("ep", None),
        P("ep", None),
        P(),
    )
    return jax.shard_map(
        body, mesh=mesh, in_specs=placed, out_specs=P(("ep", "tp"), None), check_vma=False
    )
```

```python
import functools

import jax
import jax.numpy as jnp
from jax import lax
from jax.experimental import pallas as pl
from jax.experimental.pallas import tpu as pltpu
from jax.sharding import PartitionSpec as P

norm_eps = 1.0
TOK = 144
D = 2048
HALF = 1024
SUB = 512
GROUP = 4
ROWS = GROUP * TOK

ORDER = [
    (2, 2), (1, 2), (2, 1), (2, 3),
    (3, 3), (3, 2), (0, 2), (2, 0),
    (1, 1), (1, 3), (3, 1), (3, 0),
    (1, 0), (0, 1), (0, 3), (0, 0),
]
GROUPS = [12, 8, 4, 0]
PARTS = {"g3a": (0, 2), "g3b": (2, 2), "g2a": (4, 2), "g2b": (6, 2), "g1": (8, 4), "g0": (12, 4)}
SUM_ORDER = [
    ("C", "g2b"), ("relay", 1, 0, 0), ("relay", 0, 0, 1), ("relay", 1, 0, 1), ("relay", 0, 0, 0), ("C", "g1"),
    ("free", 0, 3, 0), ("free", 1, 3, 0), ("free", 0, 0, 1), ("free", 0, 1, 0), ("free", 0, 1, 1), ("free", 1, 1, 0),
    ("free", 1, 1, 1), ("C", "g0"), ("free", 0, 0, 0), ("free", 1, 0, 0), ("free", 1, 0, 1), ("pass", 0, 0, 1),
    ("pass", 1, 0, 1), ("pass", 1, 0, 0), ("pass", 0, 0, 0), ("C", "g2a"), ("free", 0, 2, 1), ("relay", 1, 3, 0),
    ("relay", 1, 3, 1), ("free", 1, 3, 1), ("free", 0, 3, 1), ("C", "x"), ("C", "y"), ("C", "g3a"),
    ("relay", 0, 2, 0), ("relay", 0, 2, 1), ("relay", 1, 2, 0), ("relay", 1, 2, 1), ("free", 0, 2, 0),
    ("relay", 1, 1, 1), ("relay", 1, 1, 0), ("C", "g3b"), ("relay", 0, 3, 0), ("relay", 0, 3, 1), ("free", 1, 2, 0),
    ("free", 1, 2, 1), ("collect", 0, 0, 0), ("relay", 0, 1, 1), ("relay", 0, 1, 0), ("collect", 1, 0, 0),
    ("S", "near"), ("pass", 1, 3, 1), ("pass", 1, 3, 0), ("pass", 0, 2, 0), ("pass", 1, 2, 0), ("pass", 0, 2, 1),
    ("pass", 1, 2, 1), ("pass", 0, 3, 1), ("pass", 1, 1, 0), ("pass", 1, 1, 1), ("pass", 0, 3, 0), ("pass", 0, 1, 1),
    ("S", "far"), ("pass", 0, 1, 0), ("collect", 1, 3, 0), ("free2", 1, 0, 1), ("S", "work"), ("collect", 0, 2, 0),
    ("relay2", 0, 0, 0), ("relay2", 0, 0, 1), ("collect", 1, 2, 0), ("relay2", 1, 0, 0), ("relay2", 1, 0, 1),
    ("collect", 0, 3, 0), ("free2", 0, 0, 1), ("collect", 1, 1, 0), ("free2", 1, 0, 0), ("collect", 0, 1, 0),
    ("free2", 0, 0, 0), ("pass2", 0, 0, 0), ("pass2", 0, 0, 1), ("pass2", 1, 0, 0), ("pass2", 1, 0, 1),
    ("final", 0, 0, 0), ("final", 1, 0, 0),
]
SLOT = {place: i for i, place in enumerate(ORDER)}
DY = [0, 1, 3, 2]
DYI = {dy: i for i, dy in enumerate(DY)}
NT = (((1,), (1,)), ((), ()))


def kernel(
    tok_hbm, gain_hbm, ids_hbm, route_hbm, gate_hbm, up_hbm, down_hbm, sg_hbm, su_hbm, sd_hbm,
    side_in_hbm, side_out_hbm, sgate_hbm,
    out_ref,
    tok_ref, gain_ref, ids_ref, route_ref, side_ref, sgate_ref, in_sem,
    xs, own, wg, wu, wd, wx, wdx, sb, sp, sg, su, sd, shid, sout, hid, rl, rf, rl2, rf2, w8, wrow, wpat,
    ag_send, ag_m1, ag_f1, ag_m2, ag_f2,
    w_send, w_recv, w_fsend, w_frecv, w_dsend, w_drecv, w_loc, late_send, late_recv,
    x_send, x_recv, sb_dsend, sb_drecv,
    s_send, s_recv, s_fsend, s_frecv, s_dsend, s_drecv, s_loc,
    rs_send, rl_sem, rf_sem, rl2_sem, rf2_sem,
):
    ep = lax.axis_index("ep")
    tp = lax.axis_index("tp")
    z, x = ep // 4, ep % 4
    y, core = tp // 2, tp % 2

    def at_ep(dz, dx):
        return (((z + dz) % 4) * 4 + (x + dx) % 4, tp)

    def at_y(dy):
        return (ep, ((y + dy) % 4) * 2 + core)

    partner = (ep, tp + 1 - 2 * core)

    def along(axis, step):
        return at_ep(step, 0) if axis == "z" else at_ep(0, step)

    def remote(src, dst, send, recv, where):
        return pltpu.make_async_remote_copy(
            src_ref=src, dst_ref=dst, send_sem=send, recv_sem=recv, device_id=where,
            device_id_type=pl.DeviceIdType.MESH,
        )

    loads = [
        pltpu.make_async_copy(src, dst, in_sem.at[i])
        for i, (src, dst) in enumerate([
            (tok_hbm, tok_ref), (gain_hbm, gain_ref), (ids_hbm, ids_ref), (route_hbm, route_ref),
            (sgate_hbm, sgate_ref)])
    ]
    for c in loads:
        c.start()
    side_load = pltpu.make_async_copy(side_in_hbm, side_ref, in_sem.at[5])
    other_load = pltpu.make_async_copy(side_out_hbm, side_ref, in_sem.at[5])

    @pl.when(core == 0)
    def _():
        side_load.start()

    @pl.when(core == 1)
    def _():
        other_load.start()

    barrier = pltpu.get_barrier_semaphore()
    peers = [at_ep(*p) for p in ORDER if p != (0, 0)] + [at_y(d) for d in (1, 2, 3)] + [partner]
    for peer in peers:
        pl.semaphore_signal(barrier, inc=1, device_id=peer, device_id_type=pl.DeviceIdType.MESH)

    f32 = jnp.float32
    for c in loads:
        c.wait()
    values = tok_ref[...].astype(f32)
    scale_inv = lax.rsqrt(jnp.mean(values * values, axis=-1, keepdims=True) + norm_eps)
    normed = (values * scale_inv * gain_ref[...]).astype(jnp.bfloat16)
    own[0] = normed[:, :HALF]
    own[1] = normed[:, HALF:]
    xs[0, SLOT[0, 0]] = normed[:, :HALF]
    xs[1, SLOT[0, 0]] = normed[:, HALF:]
    expert = lax.broadcasted_iota(jnp.int32, (32, TOK), 0)
    dense_weight = jnp.zeros((32, TOK), f32)
    for k in range(8):
        dense_weight += jnp.where(ids_ref[k:k + 1, :] == expert, route_ref[k:k + 1, :], 0.0)
    w8[...] = jnp.zeros((16, 8, 128), f32)
    for e in range(32):
        w8[e // 2, pl.ds(2 * (e % 2), 1), :] = dense_weight[e:e + 1, :128]
        w8[e // 2, pl.ds(2 * (e % 2) + 1, 1), pl.ds(0, TOK - 128)] = dense_weight[e:e + 1, 128:]

    side_load.wait()
    for j in range(8):
        block = jnp.transpose(side_ref[:, pl.ds(128 * j, 128)].astype(f32)).astype(jnp.bfloat16)
        sp[2 * j] = block[:64]
        sp[2 * j + 1] = block[64:]
    top_row = lax.broadcasted_iota(jnp.int32, (16, 128), 0) == 0
    for j in range(16):
        part = sgate_ref[j:j + 1, :].astype(f32)
        wx[pl.ds(64, 16), pl.ds(128 * j, 128)] = jnp.where(top_row, part, 0.0).astype(jnp.bfloat16)
    wx[pl.ds(80, 48), :] = jnp.zeros((48, D), jnp.bfloat16)
    wdx[pl.ds(64, 64), :] = jnp.zeros((64, D), jnp.bfloat16)

    pl.semaphore_wait(barrier, len(peers))

    big = [(gate_hbm, wg), (up_hbm, wu), (down_hbm, wd)]
    w_p, w_m, w_fp, w_fm, w_d, w_l = [], [], [], [], {}, []
    for i, (src, dst) in enumerate(big):
        if i < 2:
            w_p.append(remote(src, dst.at[2 * DYI[3]], w_send.at[i, 0], w_recv.at[i, 0], at_y(1)))
            w_m.append(remote(src, dst.at[2 * DYI[1]], w_send.at[i, 1], w_recv.at[i, 1], at_y(3)))
        w_fp.append(remote(
            dst.at[2 * DYI[3], pl.ds(0, 64)], dst.at[2 * DYI[2], pl.ds(0, 64)],
            w_fsend.at[i, 0], w_frecv.at[i, 0], at_y(1)))
        w_fm.append(remote(
            dst.at[2 * DYI[1], pl.ds(64, 64)], dst.at[2 * DYI[2], pl.ds(64, 64)],
            w_fsend.at[i, 1], w_frecv.at[i, 1], at_y(3)))
        for dy in DY:
            w_d[i, dy] = remote(
                src if dy == 0 else dst.at[2 * DYI[dy]], dst.at[2 * DYI[dy] + 1],
                w_dsend.at[i, dy], w_drecv.at[i, dy], partner)
        w_l.append(pltpu.make_async_copy(src, dst.at[0], w_loc.at[i]))
    first_rows, last_rows = pl.ds(0, 64), pl.ds(64, 64)
    late_p = [
        remote(down_hbm.at[r], wd.at[2 * DYI[3], r], late_send.at[i, 0], late_recv.at[i, 0], at_y(1))
        for i, r in enumerate((first_rows, last_rows))]
    late_m = [
        remote(down_hbm.at[r], wd.at[2 * DYI[1], r], late_send.at[i, 1], late_recv.at[i, 1], at_y(3))
        for i, r in enumerate((last_rows, first_rows))]
    for i in range(2):
        w_p[i].start()
        w_m[i].start()
    for i in range(3):
        w_d[i, 0].start()
        w_l[i].start()

    axes = [("x", "z"), ("z", "x")]

    def src_slot(h, d1, d2):
        return SLOT[(d2, d1) if h == 0 else (d1, d2)]

    lo, hi = pl.ds(0, SUB), pl.ds(SUB, SUB)
    m1, f1, m2, f2 = {}, {}, {}, {}
    for h in range(2):
        a1, a2 = axes[h]
        s = functools.partial(src_slot, h)
        m1[h, 0] = remote(xs.at[h, s(0, 0)], xs.at[h, s(3, 0)], ag_send.at[h], ag_m1.at[h, 0], along(a1, 1))
        m1[h, 1] = remote(xs.at[h, s(0, 0)], xs.at[h, s(1, 0)], ag_send.at[h], ag_m1.at[h, 1], along(a1, 3))
        f1[h, 0] = remote(
            xs.at[h, s(3, 0), :, lo], xs.at[h, s(2, 0), :, lo], ag_send.at[h], ag_f1.at[h, 0], along(a1, 1))
        f1[h, 1] = remote(
            xs.at[h, s(1, 0), :, hi], xs.at[h, s(2, 0), :, hi], ag_send.at[h], ag_f1.at[h, 1], along(a1, 3))
        for d in range(4):
            m2[h, d, 0] = remote(
                xs.at[h, s(d, 0)], xs.at[h, s(d, 3)], ag_send.at[h], ag_m2.at[h, d, 0], along(a2, 1))
            m2[h, d, 1] = remote(
                xs.at[h, s(d, 0)], xs.at[h, s(d, 1)], ag_send.at[h], ag_m2.at[h, d, 1], along(a2, 3))
            f2[h, d, 0] = remote(
                xs.at[h, s(d, 3), :, lo], xs.at[h, s(d, 2), :, lo],
                ag_send.at[h], ag_f2.at[h, d, 0], along(a2, 1))
            f2[h, d, 1] = remote(
                xs.at[h, s(d, 1), :, hi], xs.at[h, s(d, 2), :, hi],
                ag_send.at[h], ag_f2.at[h, d, 1], along(a2, 3))

    both = [(h, k) for h in range(2) for k in range(2)]
    for h, k in both:
        m1[h, k].start()

    w_small, s_small = [], []
    for dz, dx in ORDER[:-1]:
        there = at_ep(dz, dx)
        mine = SLOT[(4 - dz) % 4, (4 - dx) % 4]
        w_small.append(remote(
            w8.at[there[0]], wrow.at[mine], x_send.at[0], x_recv.at[0], there))
        s_small.append(remote(
            sp.at[there[0]], sb.at[0, :, pl.ds(pl.multiple_of(ep * 128, 128), 128)],
            x_send.at[1], x_recv.at[1], there))
    for c in w_small + s_small:
        c.start()
    sb[0, :, pl.ds(pl.multiple_of(ep * 128, 128), 128)] = sp[ep]
    wrow[SLOT[0, 0]] = w8[ep]

    for h, k in both:
        m2[h, 0, k].start()

    s_p, s_m, s_fp, s_fm, s_d, s_l = [], [], [], [], {}, []
    for i, (src, dst) in enumerate([(sg_hbm, sg), (su_hbm, su), (sd_hbm, sd)]):
        s_p.append(remote(src, dst.at[2 * DYI[3]], s_send.at[i, 0], s_recv.at[i, 0], at_y(1)))
        s_m.append(remote(src, dst.at[2 * DYI[1]], s_send.at[i, 1], s_recv.at[i, 1], at_y(3)))
        s_fp.append(remote(
            dst.at[2 * DYI[3], pl.ds(0, 32)], dst.at[2 * DYI[2], pl.ds(0, 32)],
            s_fsend.at[i, 0], s_frecv.at[i, 0], at_y(1)))
        s_fm.append(remote(
            dst.at[2 * DYI[1], pl.ds(32, 32)], dst.at[2 * DYI[2], pl.ds(32, 32)],
            s_fsend.at[i, 1], s_frecv.at[i, 1], at_y(3)))
        for dy in DY:
            s_d[i, dy] = remote(
                src if dy == 0 else dst.at[2 * DYI[dy]], dst.at[2 * DYI[dy] + 1],
                s_dsend.at[i, dy], s_drecv.at[i, dy], partner)
        s_l.append(pltpu.make_async_copy(src, dst.at[0], s_loc.at[i]))

    def silu(v):
        return v / (1.0 + jnp.exp(-v))

    def both_halves(xa, xb, w):
        return lax.dot_general(xa, w[:, :HALF], NT, preferred_element_type=f32) + lax.dot_general(
            xb, w[:, HALF:], NT, preferred_element_type=f32)

    def rows_of(base):
        return (xs[0, pl.ds(base, GROUP)].reshape(ROWS, HALF), xs[1, pl.ds(base, GROUP)].reshape(ROWS, HALF))

    def hidden(base, first, count):
        pattern = wpat[pl.ds(base, GROUP)].reshape(ROWS, 128)
        w2 = jnp.concatenate([pattern, pattern], axis=1)

        def step(c, carry):
            xa, xb = rows_of(base)
            rows = pl.ds(2 * c, 2)
            gate = both_halves(xa, xb, wg[rows].reshape(256, D))
            up = both_halves(xa, xb, wu[rows].reshape(256, D))
            value = (silu(gate) * up * w2).astype(jnp.bfloat16)
            hid[pl.ds(base, GROUP), :, pl.ds(pl.multiple_of(c * 256, 256), 256)] = value.reshape(GROUP, TOK, 256)
            return carry

        lax.fori_loop(first, first + count, step, 0)

    def dense_hidden(base):
        xa, xb = rows_of(base)
        dense = both_halves(xa, xb, wx[...])
        lane = lax.broadcasted_iota(jnp.int32, (ROWS, 128), 1)
        opening = 1.0 / (1.0 + jnp.exp(-dense[:, 64:65]))
        value = jnp.where(lane < 64, silu(dense) * opening, 0.0).astype(jnp.bfloat16)
        hid[pl.ds(base, GROUP), :, pl.ds(1024, 128)] = value.reshape(GROUP, TOK, 128)

    def shared_expert():
        for c in range(2):
            rows = pl.ds(4 * c, 4)
            gate = both_halves(own[0], own[1], sg[rows].reshape(256, D))
            up = both_halves(own[0], own[1], su[rows].reshape(256, D))
            shid[:, pl.ds(256 * c, 256)] = (silu(gate) * up).astype(jnp.bfloat16)

        def step(n, carry):
            cols = pl.ds(pl.multiple_of(n * SUB, SUB), SUB)
            sout[:, cols] = jnp.dot(shid[...], sd[:, :, cols].reshape(512, SUB), preferred_element_type=f32)
            return carry

        lax.fori_loop(0, 4, step, 0)

    def shared_step(part):
        if part == "near":
            for i in range(3):
                s_p[i].wait_recv()
                s_fp[i].start()
                s_d[i, 3].start()
                s_m[i].wait_recv()
                s_fm[i].start()
                s_d[i, 1].start()
        elif part == "far":
            for i in range(3):
                s_fp[i].wait_recv()
                s_fm[i].wait_recv()
                s_d[i, 2].start()
        else:
            for i in range(3):
                s_l[i].wait()
                for dy in DY:
                    s_d[i, dy].wait_recv()
            shared_expert()

    def down(base, count):
        def step(n, carry):
            h = n // 2
            cols = pl.ds(pl.multiple_of(n * SUB, SUB), SUB)
            to = pl.ds(pl.multiple_of((n % 2) * SUB, SUB), SUB)
            rows = hid[pl.ds(base, count)].reshape(count * TOK, 1152)
            part = jnp.dot(rows[:, :1024], wd[:, :, cols].reshape(1024, SUB), preferred_element_type=f32)
            part = part + jnp.dot(rows[:, 1024:], wdx[:, cols], preferred_element_type=f32)
            xs[h, pl.ds(base, count), :, to] = part.astype(jnp.bfloat16).reshape(count, TOK, SUB)
            return carry

        lax.fori_loop(0, 4, step, 0)

    for h, k in both:
        m1[h, k].wait_recv()
        f1[h, k].start()
    for h in range(2):
        for d in (3, 1):
            for k in range(2):
                m2[h, d, k].start()

    def weights_on(i):
        w_p[i].wait_recv()
        w_fp[i].start()
        w_d[i, 3].start()
        w_m[i].wait_recv()
        w_fm[i].start()
        w_d[i, 1].start()

    def weights_far(i):
        w_fp[i].wait_recv()
        w_fm[i].wait_recv()
        w_d[i, 2].start()

    weights_on(0)

    pltpu.make_async_copy(wrow.at[pl.ds(0, 15)], wrow.at[pl.ds(0, 15)], x_recv.at[0]).wait()
    columns = jnp.transpose(wrow[...].reshape(128, 128))
    low_lane = lax.broadcasted_iota(jnp.int32, (128, 128), 1) < 64
    for i in range(16):
        first, last, c = columns, columns[:TOK - 128], 8 * i
        wpat[i, pl.ds(0, 128)] = jnp.where(low_lane, first[:, c:c + 1], first[:, c + 2:c + 3])
        wpat[i, pl.ds(128, TOK - 128)] = jnp.where(
            low_lane[:TOK - 128], last[:, c + 1:c + 2], last[:, c + 3:c + 4])

    for h, k in both:
        m2[h, 0, k].wait_recv()
        f2[h, 0, k].start()
    for i in range(2):
        w_l[i].wait()
        w_d[i, 0].wait_recv()
    hidden(GROUPS[0], 0, 1)
    for h, k in both:
        f1[h, k].wait_recv()
    for h in range(2):
        for k in range(2):
            m2[h, 2, k].start()
    pltpu.make_async_copy(
        sb.at[0, :, pl.ds(0, 1920)], sb.at[0, :, pl.ds(0, 1920)], x_recv.at[1]).wait()
    sb_cross = remote(sb.at[0], sb.at[1], sb_dsend, sb_drecv, partner)
    sb_cross.start()
    weights_on(1)
    for i in range(2):
        late_p[i].start()
        late_m[i].start()
    for h, k in both:
        m2[h, 3, k].wait_recv()
        f2[h, 3, k].start()
    for i in range(2):
        w_d[i, 1].wait_recv()
        w_d[i, 3].wait_recv()
    hidden(GROUPS[0], 1, 2)

    sb_cross.wait_recv()
    wx[pl.ds(0, 64), :] = sb[core]
    wdx[pl.ds(0, 64), :] = sb[1 - core]
    dense_hidden(GROUPS[0])
    for h, k in both:
        m2[h, 1, k].wait_recv()
        f2[h, 1, k].start()
    weights_far(0)
    hidden(GROUPS[1], 0, 3)
    weights_far(1)
    for h, k in both:
        f2[h, 0, k].wait_recv()
    for i in range(2):
        w_d[i, 2].wait_recv()
    hidden(GROUPS[0], 3, 1)
    hidden(GROUPS[1], 3, 1)
    late_p[0].wait_recv()
    w_fp[2].start()
    late_m[0].wait_recv()
    w_fm[2].start()
    for i in range(3):
        s_p[i].start()
        s_m[i].start()
    for i in range(3):
        s_d[i, 0].start()
        s_l[i].start()
    for h, k in both:
        m2[h, 2, k].wait_recv()
        f2[h, 2, k].start()
    dense_hidden(GROUPS[1])
    for h, k in both:
        f2[h, 3, k].wait_recv()
    late_p[1].wait_recv()
    w_d[2, 3].start()
    late_m[1].wait_recv()
    w_d[2, 1].start()
    hidden(GROUPS[2], 0, 4)
    weights_far(2)
    dense_hidden(GROUPS[2])
    for d in (1, 2):
        for h, k in both:
            f2[h, d, k].wait_recv()
    for h in range(2):
        pltpu.make_async_copy(xs.at[h, pl.ds(0, 15)], xs.at[h, pl.ds(0, 15)], ag_send.at[h]).wait()

    w_l[2].wait()
    for dy in DY:
        w_d[2, dy].wait_recv()

    def last_hidden(part):
        if part == "x":
            hidden(GROUPS[3], 0, 2)
        else:
            hidden(GROUPS[3], 2, 2)
            dense_hidden(GROUPS[3])

    rs_axes = [("z", "x"), ("x", "z")]

    def dst_slot(h, d1, q):
        return SLOT[(d1, q) if h == 0 else (q, d1)]

    r1, s1, e1, r2, s2, e2 = {}, {}, {}, {}, {}, {}
    halves = [lo, hi]
    for h in range(2):
        b1, b2 = rs_axes[h]
        t = functools.partial(dst_slot, h)
        for k in range(2):
            sum_cols, own_cols = halves[k], halves[1 - k]
            near, step = (1, 3)[k], (1, 3)[k]
            for q in range(4):
                to = along(b1, step)
                r1[h, q, k] = remote(
                    xs.at[h, t(2, q), :, sum_cols], rl.at[h, q, k], rs_send.at[h], rl_sem.at[h, q, k], to)
                s1[h, q, k] = remote(
                    xs.at[h, t(near, q), :, sum_cols], rf.at[h, q, k, :, sum_cols],
                    rs_send.at[h], rf_sem.at[h, q, k, 0], to)
                e1[h, q, k] = remote(
                    xs.at[h, t(near, q), :, own_cols], rf.at[h, q, k, :, own_cols],
                    rs_send.at[h], rf_sem.at[h, q, k, 1], to)
            to = along(b2, step)
            r2[h, k] = remote(
                xs.at[h, t(0, 2), :, sum_cols], rl2.at[h, k], rs_send.at[h], rl2_sem.at[h, k], to)
            s2[h, k] = remote(
                xs.at[h, t(0, near), :, sum_cols], rf2.at[h, k, :, sum_cols],
                rs_send.at[h], rf2_sem.at[h, k, 0], to)
            e2[h, k] = remote(
                xs.at[h, t(0, near), :, own_cols], rf2.at[h, k, :, own_cols],
                rs_send.at[h], rf2_sem.at[h, k, 1], to)

    def add(slot, h, cols, *more):
        total = xs[h, slot, :, cols].astype(f32)
        for m in more:
            total = total + m.astype(f32)
        xs[h, slot, :, cols] = total.astype(jnp.bfloat16)

    for op in SUM_ORDER:
        name = op[0]
        if name == "C":
            if op[1] in PARTS:
                down(*PARTS[op[1]])
            else:
                last_hidden(op[1])
            continue
        if name == "S":
            shared_step(op[1])
            continue
        _, h, q, k = op
        near = (1, 3)[k]
        if name == "relay":
            r1[h, q, k].start()
        elif name == "free":
            e1[h, q, k].start()
        elif name == "pass":
            r1[h, q, k].wait_recv()
            add(dst_slot(h, near, q), h, halves[k], rl[h, q, k])
            s1[h, q, k].start()
        elif name == "collect":
            for i in range(2):
                e1[h, q, i].wait_recv()
                s1[h, q, i].wait_recv()
            add(dst_slot(h, 0, q), h, pl.ds(0, HALF), rf[h, q, 0], rf[h, q, 1])
        elif name == "relay2":
            r2[h, k].start()
        elif name == "free2":
            e2[h, k].start()
        elif name == "pass2":
            r2[h, k].wait_recv()
            add(dst_slot(h, 0, near), h, halves[k], rl2[h, k])
            s2[h, k].start()
        else:
            for i in range(2):
                e2[h, i].wait_recv()
                s2[h, i].wait_recv()
            total = xs[h, SLOT[0, 0]].astype(f32) + rf2[h, 0].astype(f32) + rf2[h, 1].astype(f32)
            total = total + sout[:, pl.ds(h * HALF, HALF)]
            out_ref[:, pl.ds(h * HALF, HALF)] = total.astype(jnp.bfloat16)

    for h in range(2):
        pltpu.make_async_copy(xs.at[h, pl.ds(0, 15)], xs.at[h, pl.ds(0, 15)], rs_send.at[h]).wait()
    for i in range(2):
        w_p[i].wait_send()
        w_m[i].wait_send()
        late_p[i].wait_send()
        late_m[i].wait_send()
    for i in range(3):
        w_fp[i].wait_send()
        w_fm[i].wait_send()
        s_p[i].wait_send()
        s_m[i].wait_send()
        s_fp[i].wait_send()
        s_fm[i].wait_send()
        for dy in DY:
            w_d[i, dy].wait_send()
            s_d[i, dy].wait_send()
    pltpu.make_async_copy(wrow.at[pl.ds(0, 15)], wrow.at[pl.ds(0, 15)], x_send.at[0]).wait()
    pltpu.make_async_copy(
        sb.at[0, :, pl.ds(0, 1920)], sb.at[0, :, pl.ds(0, 1920)], x_send.at[1]).wait()
    sb_cross.wait_send()


def body(
    tokens, norm_gain, expert_ids, route_weights, expert_gate, expert_up, expert_down,
    shared_gate, shared_up, shared_down, side_in, side_out, side_gate,
):
    bf16, f32 = jnp.bfloat16, jnp.float32
    dma, vmem = pltpu.SemaphoreType.DMA, pltpu.VMEM
    in_vmem = pl.BlockSpec(memory_space=pltpu.VMEM)
    in_any = pl.BlockSpec(memory_space=pl.ANY)
    return pl.pallas_call(
        kernel,
        out_shape=pltpu.VMEM((TOK, D), bf16),
        in_specs=[in_any] * 13,
        out_specs=in_vmem,
        scratch_shapes=[
            vmem((TOK, D), bf16),
            vmem((1, D), f32),
            vmem((8, TOK), jnp.int32),
            vmem((8, TOK), f32),
            vmem((128, 1024), bf16),
            vmem((16, 128), bf16),
            dma((6,)),
            vmem((2, 16, TOK, HALF), bf16),
            vmem((2, TOK, HALF), bf16),
            vmem((8, 128, D), bf16),
            vmem((8, 128, D), bf16),
            vmem((8, 128, D), bf16),
            vmem((128, D), bf16),
            vmem((128, D), bf16),
            vmem((2, 64, D), bf16),
            vmem((16, 64, 128), bf16),
            vmem((8, 64, D), bf16),
            vmem((8, 64, D), bf16),
            vmem((8, 64, D), bf16),
            vmem((TOK, 512), bf16),
            vmem((TOK, D), f32),
            vmem((16, TOK, 1152), bf16),
            vmem((2, 4, 2, TOK, SUB), bf16),
            vmem((2, 4, 2, TOK, HALF), bf16),
            vmem((2, 2, TOK, SUB), bf16),
            vmem((2, 2, TOK, HALF), bf16),
            vmem((16, 8, 128), f32),
            vmem((16, 8, 128), f32),
            vmem((16, TOK, 128), f32),
            dma((2,)), dma((2, 2)), dma((2, 2)), dma((2, 4, 2)), dma((2, 4, 2)),
            dma((2, 2)), dma((2, 2)), dma((3, 2)), dma((3, 2)), dma((3, 4)), dma((3, 4)), dma((3,)),
            dma((2, 2)), dma((2, 2)), dma((2,)), dma((2,)), dma(()), dma(()),
            dma((3, 2)), dma((3, 2)), dma((3, 2)), dma((3, 2)), dma((3, 4)), dma((3, 4)), dma((3,)),
            dma((2,)), dma((2, 4, 2)), dma((2, 4, 2, 2)), dma((2, 2)), dma((2, 2, 2)),
        ],
        compiler_params=pltpu.CompilerParams(
            collective_id=0, has_side_effects=True, vmem_limit_bytes=60 * 1024 * 1024),
        name="routed_layer",
    )(
        tokens, norm_gain.reshape(1, D), expert_ids.T, route_weights.T,
        expert_gate.reshape(128, D), expert_up.reshape(128, D), expert_down.reshape(128, D),
        shared_gate, shared_up, shared_down, side_in, side_out, side_gate.reshape(16, 128),
    )


def solution(mesh):
    placed = (
        P(("ep", "tp"), None),
        P(),
        P(("ep", "tp"), None),
        P(("ep", "tp"), None),
        P("ep", "tp", None),
        P("ep", "tp", None),
        P("ep", "tp", None),
        P("tp", None),
        P("tp", None),
        P("tp", None),
        P("ep", None),
        P("ep", None),
        P(),
    )
    return jax.shard_map(
        body, mesh=mesh, in_specs=placed, out_specs=P(("ep", "tp"), None), check_vma=False
    )
```

```python
import functools

import jax
import jax.numpy as jnp
from jax import lax
from jax.experimental import pallas as pl
from jax.experimental.pallas import tpu as pltpu
from jax.sharding import PartitionSpec as P

norm_eps = 1.0
TOK = 144
D = 2048
HALF = 1024
SUB = 512
QUARTER = 256
GROUP = 4
ROWS = GROUP * TOK

ORDER = [
    (2, 2), (1, 2), (2, 1), (2, 3),
    (3, 3), (3, 2), (0, 2), (2, 0),
    (1, 1), (1, 3), (3, 1), (3, 0),
    (1, 0), (0, 1), (0, 3), (0, 0),
]
GROUPS = [12, 8, 4, 0]
PARTS = {"g2b": (6, 2), "g1": (8, 4), "g2a": (4, 2), "g0a": (12, 2), "g3a": (0, 2), "g0b": (14, 2), "g3b": (2, 2)}
SUM_ORDER = [
    ("C", "g2b"), ("relay", 0, 0, 1), ("relay", 0, 0, 0), ("relay", 1, 0, 0), ("relay", 1, 0, 1), ("C", "g1"),
    ("free", 0, 3, 0), ("free", 0, 1, 1), ("free", 1, 1, 1), ("free", 1, 1, 0), ("free", 1, 3, 0), ("free", 0, 1, 0),
    ("free", 0, 0, 1), ("C", "g2a"), ("relay", 1, 3, 0), ("free", 0, 2, 1), ("relay", 1, 3, 1), ("free", 0, 3, 1),
    ("free", 1, 3, 1), ("pass", 0, 0, 1), ("U", 0, 2), ("C", "g0a"), ("free", 1, 0, 0), ("free", 0, 0, 0),
    ("pass", 0, 0, 0), ("pass", 1, 0, 0), ("U", 2, 1), ("pass", 1, 3, 1), ("U", 3, 1), ("C", "g3a"),
    ("free", 0, 2, 0), ("relay", 1, 2, 0), ("relay", 0, 2, 0), ("relay", 0, 2, 1), ("relay", 1, 2, 1),
    ("relay", 1, 1, 1), ("relay", 1, 1, 0), ("pass", 1, 3, 0), ("C", "g0b"), ("pass", 1, 0, 1), ("free", 1, 0, 1),
    ("C", "g3b"), ("free", 1, 2, 0), ("relay", 0, 1, 0), ("free", 1, 2, 1), ("relay", 0, 1, 1), ("relay", 0, 3, 0),
    ("relay", 0, 3, 1), ("collect", 0, 0, 0), ("pass", 1, 2, 1), ("S", "near"), ("pass", 0, 2, 1), ("pass", 1, 2, 0),
    ("pass", 0, 2, 0), ("pass", 1, 1, 1), ("pass", 0, 1, 1), ("pass", 1, 1, 0), ("pass", 0, 1, 0), ("pass", 0, 3, 1),
    ("collect", 1, 3, 0), ("free2", 1, 0, 1), ("pass", 0, 3, 0), ("S", "far"), ("collect", 1, 0, 0), ("S", "work"),
    ("collect", 0, 2, 0), ("relay2", 0, 0, 0), ("relay2", 0, 1, 0), ("relay2", 0, 0, 1), ("relay2", 0, 1, 1),
    ("collect", 1, 2, 0), ("relay2", 1, 0, 0), ("relay2", 1, 1, 0), ("relay2", 1, 0, 1), ("relay2", 1, 1, 1),
    ("collect", 0, 1, 0), ("free2", 0, 0, 0), ("collect", 0, 3, 0), ("free2", 0, 0, 1), ("collect", 1, 1, 0),
    ("free2", 1, 0, 0), ("pass2", 0, 0, 0), ("pass2", 0, 0, 1), ("pass2", 1, 0, 0), ("pass2", 0, 1, 0),
    ("pass2", 0, 1, 1), ("pass2", 1, 1, 0), ("pass2", 1, 0, 1), ("pass2", 1, 1, 1), ("final", 0, 0, 0),
    ("final", 1, 0, 0),
]
SLOT = {place: i for i, place in enumerate(ORDER)}
DY = [0, 1, 3, 2]
DYI = {dy: i for i, dy in enumerate(DY)}
NT = (((1,), (1,)), ((), ()))


def kernel(
    tok_hbm, gain_hbm, ids_hbm, route_hbm, gate_hbm, up_hbm, down_hbm, sg_hbm, su_hbm, sd_hbm,
    side_in_hbm, side_out_hbm, sgate_hbm,
    out_ref,
    tok_ref, gain_ref, ids_ref, route_ref, side_ref, sgate_ref, in_sem,
    xs, own, wg, wu, wd, wx, wdx, sb, sp, sg, su, sd, shid, sout, hid, early, rl, rf, rl2, rf2, w8, wrow, wpat,
    ag_send, ag_m1, ag_f1, ag_m2, ag_f2,
    w_send, w_recv, w_frecv, w_drecv, w_loc, late_recv,
    x_send, x_recv, sb_dsend, sb_drecv,
    s_send, s_recv, s_frecv, s_drecv, s_loc,
    rs_send, rl_sem, rf_sem, rl2_sem, rf2_sem,
):
    ep = lax.axis_index("ep")
    tp = lax.axis_index("tp")
    z, x = ep // 4, ep % 4
    y, core = tp // 2, tp % 2

    def at_ep(dz, dx):
        return (((z + dz) % 4) * 4 + (x + dx) % 4, tp)

    def at_y(dy):
        return (ep, ((y + dy) % 4) * 2 + core)

    partner = (ep, tp + 1 - 2 * core)

    def along(axis, step):
        return at_ep(step, 0) if axis == "z" else at_ep(0, step)

    def remote(src, dst, send, recv, where):
        return pltpu.make_async_remote_copy(
            src_ref=src, dst_ref=dst, send_sem=send, recv_sem=recv, device_id=where,
            device_id_type=pl.DeviceIdType.MESH,
        )

    loads = [
        pltpu.make_async_copy(src, dst, in_sem.at[i])
        for i, (src, dst) in enumerate([
            (tok_hbm, tok_ref), (gain_hbm, gain_ref), (ids_hbm, ids_ref), (route_hbm, route_ref),
            (sgate_hbm, sgate_ref)])
    ]
    for c in loads:
        c.start()
    side_load = pltpu.make_async_copy(side_in_hbm, side_ref, in_sem.at[5])
    other_load = pltpu.make_async_copy(side_out_hbm, side_ref, in_sem.at[5])

    @pl.when(core == 0)
    def _():
        side_load.start()

    @pl.when(core == 1)
    def _():
        other_load.start()

    barrier = pltpu.get_barrier_semaphore()
    peers = [at_ep(*p) for p in ORDER if p != (0, 0)] + [at_y(d) for d in (1, 2, 3)] + [partner]
    for peer in peers:
        pl.semaphore_signal(barrier, inc=1, device_id=peer, device_id_type=pl.DeviceIdType.MESH)

    f32 = jnp.float32
    for c in loads:
        c.wait()
    values = tok_ref[...].astype(f32)
    scale_inv = lax.rsqrt(jnp.mean(values * values, axis=-1, keepdims=True) + norm_eps)
    normed = (values * scale_inv * gain_ref[...]).astype(jnp.bfloat16)
    own[0] = normed[:, :HALF]
    own[1] = normed[:, HALF:]
    xs[0, SLOT[0, 0]] = normed[:, :HALF]
    xs[1, SLOT[0, 0]] = normed[:, HALF:]
    expert = lax.broadcasted_iota(jnp.int32, (32, TOK), 0)
    dense_weight = jnp.zeros((32, TOK), f32)
    for k in range(8):
        dense_weight += jnp.where(ids_ref[k:k + 1, :] == expert, route_ref[k:k + 1, :], 0.0)
    w8[...] = jnp.zeros((16, 8, 128), f32)
    for e in range(32):
        w8[e // 2, pl.ds(2 * (e % 2), 1), :] = dense_weight[e:e + 1, :128]
        w8[e // 2, pl.ds(2 * (e % 2) + 1, 1), pl.ds(0, TOK - 128)] = dense_weight[e:e + 1, 128:]

    side_load.wait()
    for j in range(8):
        block = jnp.transpose(side_ref[:, pl.ds(128 * j, 128)].astype(f32)).astype(jnp.bfloat16)
        sp[2 * j] = block[:64]
        sp[2 * j + 1] = block[64:]
    top_row = lax.broadcasted_iota(jnp.int32, (16, 128), 0) == 0
    for j in range(16):
        part = sgate_ref[j:j + 1, :].astype(f32)
        wx[pl.ds(64, 16), pl.ds(128 * j, 128)] = jnp.where(top_row, part, 0.0).astype(jnp.bfloat16)
    wx[pl.ds(80, 48), :] = jnp.zeros((48, D), jnp.bfloat16)
    wdx[pl.ds(64, 64), :] = jnp.zeros((64, D), jnp.bfloat16)

    pl.semaphore_wait(barrier, len(peers))

    big = [(gate_hbm, wg), (up_hbm, wu), (down_hbm, wd)]
    w_p, w_m, w_fp, w_fm, w_d, w_l = [], [], [], [], {}, []
    for i, (src, dst) in enumerate(big):
        if i < 2:
            w_p.append(remote(src, dst.at[2 * DYI[3]], w_send.at[i], w_recv.at[i, 0], at_y(1)))
            w_m.append(remote(src, dst.at[2 * DYI[1]], w_send.at[i], w_recv.at[i, 1], at_y(3)))
        w_fp.append(remote(
            dst.at[2 * DYI[3], pl.ds(0, 64)], dst.at[2 * DYI[2], pl.ds(0, 64)],
            w_send.at[i], w_frecv.at[i], at_y(1)))
        w_fm.append(remote(
            dst.at[2 * DYI[1], pl.ds(64, 64)], dst.at[2 * DYI[2], pl.ds(64, 64)],
            w_send.at[i], w_frecv.at[i], at_y(3)))
        for dy in DY:
            w_d[i, dy] = remote(
                src if dy == 0 else dst.at[2 * DYI[dy]], dst.at[2 * DYI[dy] + 1],
                w_send.at[i], w_drecv.at[i, dy], partner)
        w_l.append(pltpu.make_async_copy(src, dst.at[0], w_loc.at[i]))
    first_rows, last_rows = pl.ds(0, 64), pl.ds(64, 64)
    late_p = [
        remote(down_hbm.at[r], wd.at[2 * DYI[3], r], w_send.at[2], late_recv.at[i, 0], at_y(1))
        for i, r in enumerate((first_rows, last_rows))]
    late_m = [
        remote(down_hbm.at[r], wd.at[2 * DYI[1], r], w_send.at[2], late_recv.at[i, 1], at_y(3))
        for i, r in enumerate((last_rows, first_rows))]
    for i in range(2):
        w_p[i].start()
        w_m[i].start()
    for i in range(3):
        w_d[i, 0].start()
        w_l[i].start()

    axes = [("x", "z"), ("z", "x")]

    def src_slot(h, d1, d2):
        return SLOT[(d2, d1) if h == 0 else (d1, d2)]

    lo, hi = pl.ds(0, SUB), pl.ds(SUB, SUB)
    m1, f1, m2, f2 = {}, {}, {}, {}
    for h in range(2):
        a1, a2 = axes[h]
        s = functools.partial(src_slot, h)
        m1[h, 0] = remote(xs.at[h, s(0, 0)], xs.at[h, s(3, 0)], ag_send.at[h], ag_m1.at[h, 0], along(a1, 1))
        m1[h, 1] = remote(xs.at[h, s(0, 0)], xs.at[h, s(1, 0)], ag_send.at[h], ag_m1.at[h, 1], along(a1, 3))
        f1[h, 0] = remote(
            xs.at[h, s(3, 0), :, lo], xs.at[h, s(2, 0), :, lo], ag_send.at[h], ag_f1.at[h, 0], along(a1, 1))
        f1[h, 1] = remote(
            xs.at[h, s(1, 0), :, hi], xs.at[h, s(2, 0), :, hi], ag_send.at[h], ag_f1.at[h, 1], along(a1, 3))
        for d in range(4):
            m2[h, d, 0] = remote(
                xs.at[h, s(d, 0)], xs.at[h, s(d, 3)], ag_send.at[h], ag_m2.at[h, d, 0], along(a2, 1))
            m2[h, d, 1] = remote(
                xs.at[h, s(d, 0)], xs.at[h, s(d, 1)], ag_send.at[h], ag_m2.at[h, d, 1], along(a2, 3))
            f2[h, d, 0] = remote(
                xs.at[h, s(d, 3), :, lo], xs.at[h, s(d, 2), :, lo],
                ag_send.at[h], ag_f2.at[h, d], along(a2, 1))
            f2[h, d, 1] = remote(
                xs.at[h, s(d, 1), :, hi], xs.at[h, s(d, 2), :, hi],
                ag_send.at[h], ag_f2.at[h, d], along(a2, 3))

    both = [(h, k) for h in range(2) for k in range(2)]
    for h, k in both:
        m1[h, k].start()

    w_small, s_small = [], []
    for dz, dx in ORDER[:-1]:
        there = at_ep(dz, dx)
        mine = SLOT[(4 - dz) % 4, (4 - dx) % 4]
        w_small.append(remote(
            w8.at[there[0]], wrow.at[mine], x_send.at[0], x_recv.at[0], there))
        s_small.append(remote(
            sp.at[there[0]], sb.at[0, :, pl.ds(pl.multiple_of(ep * 128, 128), 128)],
            x_send.at[1], x_recv.at[1], there))
    for c in w_small + s_small:
        c.start()
    sb[0, :, pl.ds(pl.multiple_of(ep * 128, 128), 128)] = sp[ep]
    wrow[SLOT[0, 0]] = w8[ep]

    for h, k in both:
        m2[h, 0, k].start()

    s_p, s_m, s_fp, s_fm, s_d, s_l = [], [], [], [], {}, []
    for i, (src, dst) in enumerate([(sg_hbm, sg), (su_hbm, su), (sd_hbm, sd)]):
        s_p.append(remote(src, dst.at[DYI[3]], s_send.at[i], s_recv.at[i, 0], at_y(1)))
        s_m.append(remote(src, dst.at[DYI[1]], s_send.at[i], s_recv.at[i, 1], at_y(3)))
        s_fp.append(remote(
            dst.at[DYI[3], pl.ds(0, 32)], dst.at[DYI[2], pl.ds(0, 32)],
            s_send.at[i], s_frecv.at[i], at_y(1)))
        s_fm.append(remote(
            dst.at[DYI[1], pl.ds(32, 32)], dst.at[DYI[2], pl.ds(32, 32)],
            s_send.at[i], s_frecv.at[i], at_y(3)))
        for dy in DY:
            s_d[i, dy] = remote(
                src if dy == 0 else dst.at[DYI[dy]], dst.at[4 + DYI[dy]],
                s_send.at[i], s_drecv.at[i], partner)
        s_l.append(pltpu.make_async_copy(src, dst.at[0], s_loc.at[i]))

    def silu(v):
        return v / (1.0 + jnp.exp(-v))

    def both_halves(xa, xb, w):
        return lax.dot_general(xa, w[:, :HALF], NT, preferred_element_type=f32) + lax.dot_general(
            xb, w[:, HALF:], NT, preferred_element_type=f32)

    def rows_of(base):
        return (xs[0, pl.ds(base, GROUP)].reshape(ROWS, HALF), xs[1, pl.ds(base, GROUP)].reshape(ROWS, HALF))

    def hidden(base, first, count):
        pattern = wpat[pl.ds(base, GROUP)].reshape(ROWS, 128)
        w2 = jnp.concatenate([pattern, pattern], axis=1)

        def step(c, carry):
            xa, xb = rows_of(base)
            rows = pl.ds(2 * c, 2)
            gate = both_halves(xa, xb, wg[rows].reshape(256, D))
            up = both_halves(xa, xb, wu[rows].reshape(256, D))
            value = (silu(gate) * up * w2).astype(jnp.bfloat16)
            hid[pl.ds(base, GROUP), :, pl.ds(pl.multiple_of(c * 256, 256), 256)] = value.reshape(GROUP, TOK, 256)
            return carry

        lax.fori_loop(first, first + count, step, 0)

    def dense_hidden(base):
        xa, xb = rows_of(base)
        dense = both_halves(xa, xb, wx[...])
        lane = lax.broadcasted_iota(jnp.int32, (ROWS, 128), 1)
        opening = 1.0 / (1.0 + jnp.exp(-dense[:, 64:65]))
        value = jnp.where(lane < 64, silu(dense) * opening, 0.0).astype(jnp.bfloat16)
        hid[pl.ds(base, GROUP), :, pl.ds(1024, 128)] = value.reshape(GROUP, TOK, 128)

    def shared_expert():
        for c in range(2):
            rows = pl.ds(4 * c, 4)
            gate = both_halves(own[0], own[1], sg[rows].reshape(256, D))
            up = both_halves(own[0], own[1], su[rows].reshape(256, D))
            shid[:, pl.ds(256 * c, 256)] = (silu(gate) * up).astype(jnp.bfloat16)

        def step(n, carry):
            cols = pl.ds(pl.multiple_of(n * SUB, SUB), SUB)
            sout[:, cols] = jnp.dot(shid[...], sd[:, :, cols].reshape(512, SUB), preferred_element_type=f32)
            return carry

        lax.fori_loop(0, 4, step, 0)

    def shared_step(part):
        if part == "near":
            for i in range(3):
                s_p[i].wait_recv()
                s_fp[i].start()
                s_d[i, 3].start()
                s_m[i].wait_recv()
                s_fm[i].start()
                s_d[i, 1].start()
        elif part == "far":
            for i in range(3):
                far = (sg, su, sd)[i].at[DYI[2]]
                pltpu.make_async_copy(far, far, s_frecv.at[i]).wait()
                s_d[i, 2].start()
        else:
            for i in range(3):
                s_l[i].wait()
                across = (sg, su, sd)[i].at[pl.ds(4, 4)]
                pltpu.make_async_copy(across, across, s_drecv.at[i]).wait()
            shared_expert()

    def down(base, count):
        def step(n, carry):
            h = n // 2
            cols = pl.ds(pl.multiple_of(n * SUB, SUB), SUB)
            to = pl.ds(pl.multiple_of((n % 2) * SUB, SUB), SUB)
            rows = hid[pl.ds(base, count)].reshape(count * TOK, 1152)
            part = jnp.dot(rows[:, :1024], wd[:, :, cols].reshape(1024, SUB), preferred_element_type=f32)
            part = part + jnp.dot(rows[:, 1024:], wdx[:, cols], preferred_element_type=f32)
            xs[h, pl.ds(base, count), :, to] = part.astype(jnp.bfloat16).reshape(count, TOK, SUB)
            return carry

        lax.fori_loop(0, 4, step, 0)

    def down_early(base):
        def step(n, carry):
            cols = pl.ds(pl.multiple_of(n * SUB, SUB), SUB)
            rows = hid[pl.ds(base, 2)].reshape(2 * TOK, 1152)
            part = jnp.dot(
                rows[:, :768], wd[pl.ds(0, 6), :, cols].reshape(768, SUB), preferred_element_type=f32)
            early[:, cols] = part + jnp.dot(rows[:, 1024:], wdx[:, cols], preferred_element_type=f32)
            return carry

        lax.fori_loop(0, 4, step, 0)

    def down_late(base):
        def step(n, carry):
            h = n // 2
            cols = pl.ds(pl.multiple_of(n * SUB, SUB), SUB)
            to = pl.ds(pl.multiple_of((n % 2) * SUB, SUB), SUB)
            rows = hid[pl.ds(base, 2)].reshape(2 * TOK, 1152)
            part = early[:, cols] + jnp.dot(
                rows[:, 768:1024], wd[pl.ds(6, 2), :, cols].reshape(256, SUB), preferred_element_type=f32)
            xs[h, pl.ds(base, 2), :, to] = part.astype(jnp.bfloat16).reshape(2, TOK, SUB)
            return carry

        lax.fori_loop(0, 4, step, 0)

    for h, k in both:
        m1[h, k].wait_recv()
        f1[h, k].start()
    for h in range(2):
        for d in (3, 1):
            for k in range(2):
                m2[h, d, k].start()

    def weights_on(i):
        w_p[i].wait_recv()
        w_fp[i].start()
        w_d[i, 3].start()
        w_m[i].wait_recv()
        w_fm[i].start()
        w_d[i, 1].start()

    def far_rows(d):
        for h in range(2):
            here = xs.at[h, src_slot(h, d, 2)]
            pltpu.make_async_copy(here, here, ag_f2.at[h, d]).wait()

    def weights_far(i):
        far = (wg, wu, wd)[i].at[2 * DYI[2]]
        pltpu.make_async_copy(far, far, w_frecv.at[i]).wait()
        w_d[i, 2].start()

    weights_on(0)

    pltpu.make_async_copy(wrow.at[pl.ds(0, 15)], wrow.at[pl.ds(0, 15)], x_recv.at[0]).wait()
    columns = jnp.transpose(wrow[...].reshape(128, 128))
    low_lane = lax.broadcasted_iota(jnp.int32, (128, 128), 1) < 64
    for i in range(16):
        first, last, c = columns, columns[:TOK - 128], 8 * i
        wpat[i, pl.ds(0, 128)] = jnp.where(low_lane, first[:, c:c + 1], first[:, c + 2:c + 3])
        wpat[i, pl.ds(128, TOK - 128)] = jnp.where(
            low_lane[:TOK - 128], last[:, c + 1:c + 2], last[:, c + 3:c + 4])

    for h, k in both:
        m2[h, 0, k].wait_recv()
        f2[h, 0, k].start()
    for i in range(2):
        w_l[i].wait()
        w_d[i, 0].wait_recv()
    hidden(GROUPS[0], 0, 1)
    for h, k in both:
        f1[h, k].wait_recv()
    for h in range(2):
        for k in range(2):
            m2[h, 2, k].start()
    pltpu.make_async_copy(
        sb.at[0, :, pl.ds(0, 1920)], sb.at[0, :, pl.ds(0, 1920)], x_recv.at[1]).wait()
    sb_cross = remote(sb.at[0], sb.at[1], sb_dsend, sb_drecv, partner)
    sb_cross.start()
    weights_on(1)
    for i in range(2):
        late_p[i].start()
        late_m[i].start()
    for h, k in both:
        m2[h, 3, k].wait_recv()
        f2[h, 3, k].start()
    for i in range(2):
        w_d[i, 1].wait_recv()
        w_d[i, 3].wait_recv()
    hidden(GROUPS[0], 1, 2)

    sb_cross.wait_recv()
    wx[pl.ds(0, 64), :] = sb[core]
    wdx[pl.ds(0, 64), :] = sb[1 - core]
    dense_hidden(GROUPS[0])
    for h, k in both:
        m2[h, 1, k].wait_recv()
        f2[h, 1, k].start()
    weights_far(0)
    hidden(GROUPS[1], 0, 3)
    weights_far(1)
    far_rows(0)
    for i in range(2):
        w_d[i, 2].wait_recv()
    hidden(GROUPS[0], 3, 1)
    hidden(GROUPS[1], 3, 1)
    late_p[0].wait_recv()
    w_fp[2].start()
    late_m[0].wait_recv()
    w_fm[2].start()
    for i in range(3):
        s_p[i].start()
        s_m[i].start()
    for i in range(3):
        s_d[i, 0].start()
        s_l[i].start()
    for h, k in both:
        m2[h, 2, k].wait_recv()
        f2[h, 2, k].start()
    dense_hidden(GROUPS[1])
    far_rows(3)
    hidden(GROUPS[2], 0, 2)
    late_p[1].wait_recv()
    w_d[2, 3].start()
    late_m[1].wait_recv()
    w_d[2, 1].start()
    hidden(GROUPS[2], 2, 2)
    dense_hidden(GROUPS[2])
    weights_far(2)
    w_l[2].wait()
    for dy in (0, 1, 3):
        w_d[2, dy].wait_recv()
    down_early(PARTS["g2b"][0])
    far_rows(1)
    far_rows(2)
    for h in range(2):
        pltpu.make_async_copy(xs.at[h, pl.ds(0, 15)], xs.at[h, pl.ds(0, 15)], ag_send.at[h]).wait()
    w_d[2, 2].wait_recv()

    rs_axes = [("z", "x"), ("x", "z")]

    def dst_slot(h, d1, q):
        return SLOT[(d1, q) if h == 0 else (q, d1)]

    r1, s1, e1, r2, s2, e2 = {}, {}, {}, {}, {}, {}
    halves = [lo, hi]
    for h in range(2):
        b1, b2 = rs_axes[h]
        t = functools.partial(dst_slot, h)
        for k in range(2):
            sum_cols, own_cols = halves[k], halves[1 - k]
            near, step = (1, 3)[k], (1, 3)[k]
            for q in range(4):
                to = along(b1, step)
                r1[h, q, k] = remote(
                    xs.at[h, t(2, q), :, sum_cols], rl.at[h, q, k], rs_send.at[h], rl_sem.at[h, q, k], to)
                s1[h, q, k] = remote(
                    xs.at[h, t(near, q), :, sum_cols], rf.at[h, q, k, :, sum_cols],
                    rs_send.at[h], rf_sem.at[h, q], to)
                e1[h, q, k] = remote(
                    xs.at[h, t(near, q), :, own_cols], rf.at[h, q, k, :, own_cols],
                    rs_send.at[h], rf_sem.at[h, q], to)
            to = along(b2, step)
            for p in range(2):
                cols = pl.ds(SUB * k + QUARTER * p, QUARTER)
                r2[h, p, k] = remote(
                    xs.at[h, t(0, 2), :, cols], rl2.at[h, k, :, pl.ds(QUARTER * p, QUARTER)],
                    rs_send.at[h], rl2_sem.at[h, p, k], to)
                s2[h, p, k] = remote(
                    xs.at[h, t(0, near), :, cols], rf2.at[h, k, :, cols],
                    rs_send.at[h], rf2_sem.at[h, k, p], to)
            e2[h, k] = remote(
                xs.at[h, t(0, near), :, own_cols], rf2.at[h, k, :, own_cols],
                rs_send.at[h], rf2_sem.at[h, k, 2], to)

    def add(slot, h, cols, *more):
        total = xs[h, slot, :, cols].astype(f32)
        for m in more:
            total = total + m.astype(f32)
        xs[h, slot, :, cols] = total.astype(jnp.bfloat16)

    for op in SUM_ORDER:
        name = op[0]
        if name == "C":
            if op[1] == "g2b":
                down_late(PARTS["g2b"][0])
            else:
                down(*PARTS[op[1]])
            continue
        if name == "U":
            hidden(GROUPS[3], op[1], op[2])
            if op[1] + op[2] == 4:
                dense_hidden(GROUPS[3])
            continue
        if name == "S":
            shared_step(op[1])
            continue
        _, h, q, k = op
        near = (1, 3)[k]
        if name == "relay":
            r1[h, q, k].start()
        elif name == "free":
            e1[h, q, k].start()
        elif name == "pass":
            r1[h, q, k].wait_recv()
            add(dst_slot(h, near, q), h, halves[k], rl[h, q, k])
            s1[h, q, k].start()
        elif name == "collect":
            pltpu.make_async_copy(rf.at[h, q], rf.at[h, q], rf_sem.at[h, q]).wait()
            add(dst_slot(h, 0, q), h, pl.ds(0, HALF), rf[h, q, 0], rf[h, q, 1])
        elif name == "relay2":
            r2[h, q, k].start()
        elif name == "free2":
            e2[h, k].start()
        elif name == "pass2":
            r2[h, q, k].wait_recv()
            add(
                dst_slot(h, 0, near), h, pl.ds(SUB * k + QUARTER * q, QUARTER),
                rl2[h, k, :, pl.ds(QUARTER * q, QUARTER)])
            s2[h, q, k].start()
        else:
            for i in range(2):
                e2[h, i].wait_recv()
                s2[h, 0, i].wait_recv()
                s2[h, 1, i].wait_recv()
            total = xs[h, SLOT[0, 0]].astype(f32) + rf2[h, 0].astype(f32) + rf2[h, 1].astype(f32)
            total = total + sout[:, pl.ds(h * HALF, HALF)]
            out_ref[:, pl.ds(h * HALF, HALF)] = total.astype(jnp.bfloat16)

    for h in range(2):
        pltpu.make_async_copy(xs.at[h, pl.ds(0, 15)], xs.at[h, pl.ds(0, 15)], rs_send.at[h]).wait()
    for sent, sem in ((wg, w_send.at[0]), (wu, w_send.at[1]), (wd, w_send.at[2])):
        pltpu.make_async_copy(sent.at[pl.ds(0, 7)], sent.at[pl.ds(0, 7)], sem).wait()
    for i, sent in enumerate((sg, su, sd)):
        pltpu.make_async_copy(sent.at[pl.ds(0, 7)], sent.at[pl.ds(0, 7)], s_send.at[i]).wait()
    pltpu.make_async_copy(wrow.at[pl.ds(0, 15)], wrow.at[pl.ds(0, 15)], x_send.at[0]).wait()
    pltpu.make_async_copy(
        sb.at[0, :, pl.ds(0, 1920)], sb.at[0, :, pl.ds(0, 1920)], x_send.at[1]).wait()
    sb_cross.wait_send()


def body(
    tokens, norm_gain, expert_ids, route_weights, expert_gate, expert_up, expert_down,
    shared_gate, shared_up, shared_down, side_in, side_out, side_gate,
):
    bf16, f32 = jnp.bfloat16, jnp.float32
    dma, vmem = pltpu.SemaphoreType.DMA, pltpu.VMEM
    in_vmem = pl.BlockSpec(memory_space=pltpu.VMEM)
    in_any = pl.BlockSpec(memory_space=pl.ANY)
    return pl.pallas_call(
        kernel,
        out_shape=pltpu.VMEM((TOK, D), bf16),
        in_specs=[in_any] * 13,
        out_specs=in_vmem,
        scratch_shapes=[
            vmem((TOK, D), bf16),
            vmem((1, D), f32),
            vmem((8, TOK), jnp.int32),
            vmem((8, TOK), f32),
            vmem((128, 1024), bf16),
            vmem((16, 128), bf16),
            dma((6,)),
            vmem((2, 16, TOK, HALF), bf16),
            vmem((2, TOK, HALF), bf16),
            vmem((8, 128, D), bf16),
            vmem((8, 128, D), bf16),
            vmem((8, 128, D), bf16),
            vmem((128, D), bf16),
            vmem((128, D), bf16),
            vmem((2, 64, D), bf16),
            vmem((16, 64, 128), bf16),
            vmem((8, 64, D), bf16),
            vmem((8, 64, D), bf16),
            vmem((8, 64, D), bf16),
            vmem((TOK, 512), bf16),
            vmem((TOK, D), f32),
            vmem((16, TOK, 1152), bf16),
            vmem((2 * TOK, D), f32),
            vmem((2, 4, 2, TOK, SUB), bf16),
            vmem((2, 4, 2, TOK, HALF), bf16),
            vmem((2, 2, TOK, SUB), bf16),
            vmem((2, 2, TOK, HALF), bf16),
            vmem((16, 8, 128), f32),
            vmem((16, 8, 128), f32),
            vmem((16, TOK, 128), f32),
            dma((2,)), dma((2, 2)), dma((2, 2)), dma((2, 4, 2)), dma((2, 4)),
            dma((3,)), dma((2, 2)), dma((3,)), dma((3, 4)), dma((3,)), dma((2, 2)),
            dma((2,)), dma((2,)), dma(()), dma(()),
            dma((3,)), dma((3, 2)), dma((3,)), dma((3,)), dma((3,)),
            dma((2,)), dma((2, 4, 2)), dma((2, 4)), dma((2, 2, 2)), dma((2, 2, 3)),
        ],
        compiler_params=pltpu.CompilerParams(
            collective_id=0, has_side_effects=True, vmem_limit_bytes=60 * 1024 * 1024),
        name="routed_layer",
    )(
        tokens, norm_gain.reshape(1, D), expert_ids.T, route_weights.T,
        expert_gate.reshape(128, D), expert_up.reshape(128, D), expert_down.reshape(128, D),
        shared_gate, shared_up, shared_down, side_in, side_out, side_gate.reshape(16, 128),
    )


def solution(mesh):
    placed = (
        P(("ep", "tp"), None),
        P(),
        P(("ep", "tp"), None),
        P(("ep", "tp"), None),
        P("ep", "tp", None),
        P("ep", "tp", None),
        P("ep", "tp", None),
        P("tp", None),
        P("tp", None),
        P("tp", None),
        P("ep", None),
        P("ep", None),
        P(),
    )
    return jax.shard_map(
        body, mesh=mesh, in_specs=placed, out_specs=P(("ep", "tp"), None), check_vma=False
    )
```

```python
import functools

import jax
import jax.numpy as jnp
from jax import lax
from jax.experimental import pallas as pl
from jax.experimental.pallas import tpu as pltpu
from jax.sharding import PartitionSpec as P

norm_eps = 1.0
TOK = 144
D = 2048
HALF = 1024
SUB = 512
QUARTER = 256
GROUP = 4
ROWS = GROUP * TOK

ORDER = [
    (2, 2), (1, 2), (2, 1), (2, 3),
    (3, 3), (3, 2), (0, 2), (2, 0),
    (1, 1), (1, 3), (3, 1), (3, 0),
    (1, 0), (0, 1), (0, 3), (0, 0),
]
GROUPS = [12, 8, 4, 0]
PARTS = {"g2b": (6, 2), "g1": (8, 4), "g2a": (4, 2), "g0a": (12, 2), "g3a": (0, 2), "g0b": (14, 2), "g3b": (2, 2)}
SUM_ORDER = [
    ("C", "g2b"), ("relay", 0, 0, 1), ("relay", 0, 0, 0), ("relay", 1, 0, 0), ("relay", 1, 0, 1), ("C", "g1"),
    ("free", 0, 3, 0), ("free", 0, 1, 1), ("free", 1, 1, 1), ("free", 1, 1, 0), ("free", 1, 3, 0), ("free", 0, 1, 0),
    ("free", 0, 0, 1), ("C", "g2a"), ("relay", 1, 3, 0), ("free", 0, 2, 1), ("relay", 1, 3, 1), ("free", 0, 3, 1),
    ("free", 1, 3, 1), ("pass", 0, 0, 1), ("U", 0, 2), ("C", "g0a"), ("free", 1, 0, 0), ("free", 0, 0, 0),
    ("pass", 0, 0, 0), ("pass", 1, 0, 0), ("U", 2, 2), ("pass", 1, 3, 1), ("C", "g3a"), ("free", 0, 2, 0),
    ("relay", 1, 2, 0), ("relay", 0, 2, 0), ("relay", 0, 2, 1), ("relay", 1, 2, 1), ("relay", 1, 1, 1),
    ("relay", 1, 1, 0), ("pass", 1, 3, 0), ("C", "g0b"), ("pass", 1, 0, 1), ("free", 1, 0, 1), ("C", "g3b"),
    ("free", 1, 2, 0), ("relay", 0, 1, 0), ("free", 1, 2, 1), ("relay", 0, 1, 1), ("relay", 0, 3, 0),
    ("relay", 0, 3, 1), ("collect", 0, 0, 0), ("pass", 1, 2, 1), ("S", "near"), ("pass", 0, 2, 1), ("pass", 1, 2, 0),
    ("pass", 0, 2, 0), ("pass", 1, 1, 1), ("pass", 0, 1, 1), ("pass", 1, 1, 0), ("pass", 0, 1, 0), ("pass", 0, 3, 1),
    ("collect", 1, 3, 0), ("free2", 1, 0, 1), ("pass", 0, 3, 0), ("S", "far"), ("collect", 1, 0, 0), ("S", "work"),
    ("collect", 0, 2, 0), ("relay2", 0, 0, 0), ("relay2", 0, 1, 0), ("relay2", 0, 0, 1), ("relay2", 0, 1, 1),
    ("collect", 1, 2, 0), ("relay2", 1, 0, 0), ("relay2", 1, 1, 0), ("relay2", 1, 0, 1), ("relay2", 1, 1, 1),
    ("collect", 0, 1, 0), ("free2", 0, 0, 0), ("collect", 0, 3, 0), ("free2", 0, 0, 1), ("collect", 1, 1, 0),
    ("free2", 1, 0, 0), ("pass2", 0, 0, 0), ("pass2", 0, 0, 1), ("pass2", 1, 0, 0), ("pass2", 0, 1, 0),
    ("pass2", 0, 1, 1), ("pass2", 1, 1, 0), ("pass2", 1, 0, 1), ("pass2", 1, 1, 1), ("final", 0, 0, 0),
    ("final", 1, 0, 0),
]
SLOT = {place: i for i, place in enumerate(ORDER)}
DY = [0, 1, 3, 2]
DYI = {dy: i for i, dy in enumerate(DY)}
NT = (((1,), (1,)), ((), ()))


def kernel(
    tok_hbm, gain_hbm, ids_hbm, route_hbm, gate_hbm, up_hbm, down_hbm, sg_hbm, su_hbm, sd_hbm,
    side_in_hbm, side_out_hbm, sgate_hbm,
    out_ref,
    tok_ref, gain_ref, ids_ref, route_ref, side_ref, sgate_ref, in_sem,
    xs, own, wg, wu, wd, wx, wdx, sb, sp, sg, su, sd, shid, sout, hid, early, rl, rf, rl2, rf2, w8, wrow, wpat,
    ag_send, ag_m1, ag_f1, ag_m2, ag_f2,
    w_send, w_recv, w_frecv, w_drecv, w_loc, late_recv,
    x_send, x_recv, sb_dsend, sb_drecv,
    s_send, s_recv, s_frecv, s_drecv, s_loc,
    rs_send, rl_sem, rf_sem, rl2_sem, rf2_sem,
):
    ep = lax.axis_index("ep")
    tp = lax.axis_index("tp")
    z, x = ep // 4, ep % 4
    y, core = tp // 2, tp % 2

    def at_ep(dz, dx):
        return (((z + dz) % 4) * 4 + (x + dx) % 4, tp)

    def at_y(dy):
        return (ep, ((y + dy) % 4) * 2 + core)

    partner = (ep, tp + 1 - 2 * core)

    def along(axis, step):
        return at_ep(step, 0) if axis == "z" else at_ep(0, step)

    def remote(src, dst, send, recv, where):
        return pltpu.make_async_remote_copy(
            src_ref=src, dst_ref=dst, send_sem=send, recv_sem=recv, device_id=where,
            device_id_type=pl.DeviceIdType.MESH,
        )

    loads = [
        pltpu.make_async_copy(src, dst, in_sem.at[i])
        for i, (src, dst) in enumerate([
            (tok_hbm, tok_ref), (gain_hbm, gain_ref), (ids_hbm, ids_ref), (route_hbm, route_ref),
            (sgate_hbm, sgate_ref)])
    ]
    for c in loads:
        c.start()
    side_load = pltpu.make_async_copy(side_in_hbm, side_ref, in_sem.at[5])
    other_load = pltpu.make_async_copy(side_out_hbm, side_ref, in_sem.at[5])

    @pl.when(core == 0)
    def _():
        side_load.start()

    @pl.when(core == 1)
    def _():
        other_load.start()

    barrier = pltpu.get_barrier_semaphore()
    peers = [at_ep(*p) for p in ORDER if p != (0, 0)] + [at_y(d) for d in (1, 2, 3)] + [partner]
    for peer in peers:
        pl.semaphore_signal(barrier, inc=1, device_id=peer, device_id_type=pl.DeviceIdType.MESH)

    f32 = jnp.float32
    for c in loads:
        c.wait()
    values = tok_ref[...].astype(f32)
    scale_inv = lax.rsqrt(jnp.mean(values * values, axis=-1, keepdims=True) + norm_eps)
    normed = (values * scale_inv * gain_ref[...]).astype(jnp.bfloat16)
    own[0] = normed[:, :HALF]
    own[1] = normed[:, HALF:]
    xs[0, SLOT[0, 0]] = normed[:, :HALF]
    xs[1, SLOT[0, 0]] = normed[:, HALF:]
    expert = lax.broadcasted_iota(jnp.int32, (32, TOK), 0)
    dense_weight = jnp.zeros((32, TOK), f32)
    for k in range(8):
        dense_weight += jnp.where(ids_ref[k:k + 1, :] == expert, route_ref[k:k + 1, :], 0.0)
    w8[...] = jnp.zeros((16, 8, 128), f32)
    for e in range(32):
        w8[e // 2, pl.ds(2 * (e % 2), 1), :] = dense_weight[e:e + 1, :128]
        w8[e // 2, pl.ds(2 * (e % 2) + 1, 1), pl.ds(0, TOK - 128)] = dense_weight[e:e + 1, 128:]

    side_load.wait()
    for j in range(8):
        block = jnp.transpose(side_ref[:, pl.ds(128 * j, 128)].astype(f32)).astype(jnp.bfloat16)
        sp[2 * j] = block[:64]
        sp[2 * j + 1] = block[64:]
    top_row = lax.broadcasted_iota(jnp.int32, (16, 128), 0) == 0
    for j in range(16):
        part = sgate_ref[j:j + 1, :].astype(f32)
        wx[pl.ds(64, 16), pl.ds(128 * j, 128)] = jnp.where(top_row, part, 0.0).astype(jnp.bfloat16)
    wx[pl.ds(80, 48), :] = jnp.zeros((48, D), jnp.bfloat16)
    wdx[pl.ds(64, 64), :] = jnp.zeros((64, D), jnp.bfloat16)

    pl.semaphore_wait(barrier, len(peers))

    big = [(gate_hbm, wg), (up_hbm, wu), (down_hbm, wd)]
    w_p, w_m, w_fp, w_fm, w_d, w_l = [], [], [], [], {}, []
    for i, (src, dst) in enumerate(big):
        if i < 2:
            w_p.append(remote(src, dst.at[2 * DYI[3]], w_send.at[i], w_recv.at[i, 0], at_y(1)))
            w_m.append(remote(src, dst.at[2 * DYI[1]], w_send.at[i], w_recv.at[i, 1], at_y(3)))
        w_fp.append(remote(
            dst.at[2 * DYI[3], pl.ds(0, 64)], dst.at[2 * DYI[2], pl.ds(0, 64)],
            w_send.at[i], w_frecv.at[i], at_y(1)))
        w_fm.append(remote(
            dst.at[2 * DYI[1], pl.ds(64, 64)], dst.at[2 * DYI[2], pl.ds(64, 64)],
            w_send.at[i], w_frecv.at[i], at_y(3)))
        for dy in DY:
            w_d[i, dy] = remote(
                src if dy == 0 else dst.at[2 * DYI[dy]], dst.at[2 * DYI[dy] + 1],
                w_send.at[i], w_drecv.at[i, dy], partner)
        w_l.append(pltpu.make_async_copy(src, dst.at[0], w_loc.at[i]))
    first_rows, last_rows = pl.ds(0, 64), pl.ds(64, 64)
    late_p = [
        remote(down_hbm.at[r], wd.at[2 * DYI[3], r], w_send.at[2], late_recv.at[i, 0], at_y(1))
        for i, r in enumerate((first_rows, last_rows))]
    late_m = [
        remote(down_hbm.at[r], wd.at[2 * DYI[1], r], w_send.at[2], late_recv.at[i, 1], at_y(3))
        for i, r in enumerate((last_rows, first_rows))]
    for i in range(2):
        w_p[i].start()
        w_m[i].start()
    for i in range(3):
        w_d[i, 0].start()
        w_l[i].start()

    axes = [("x", "z"), ("z", "x")]

    def src_slot(h, d1, d2):
        return SLOT[(d2, d1) if h == 0 else (d1, d2)]

    lo, hi = pl.ds(0, SUB), pl.ds(SUB, SUB)
    m1, f1, m2, f2 = {}, {}, {}, {}
    for h in range(2):
        a1, a2 = axes[h]
        s = functools.partial(src_slot, h)
        m1[h, 0] = remote(xs.at[h, s(0, 0)], xs.at[h, s(3, 0)], ag_send.at[h], ag_m1.at[h, 0], along(a1, 1))
        m1[h, 1] = remote(xs.at[h, s(0, 0)], xs.at[h, s(1, 0)], ag_send.at[h], ag_m1.at[h, 1], along(a1, 3))
        f1[h, 0] = remote(
            xs.at[h, s(3, 0), :, lo], xs.at[h, s(2, 0), :, lo], ag_send.at[h], ag_f1.at[h, 0], along(a1, 1))
        f1[h, 1] = remote(
            xs.at[h, s(1, 0), :, hi], xs.at[h, s(2, 0), :, hi], ag_send.at[h], ag_f1.at[h, 1], along(a1, 3))
        for d in range(4):
            m2[h, d, 0] = remote(
                xs.at[h, s(d, 0)], xs.at[h, s(d, 3)], ag_send.at[h], ag_m2.at[h, d, 0], along(a2, 1))
            m2[h, d, 1] = remote(
                xs.at[h, s(d, 0)], xs.at[h, s(d, 1)], ag_send.at[h], ag_m2.at[h, d, 1], along(a2, 3))
            f2[h, d, 0] = remote(
                xs.at[h, s(d, 3), :, lo], xs.at[h, s(d, 2), :, lo],
                ag_send.at[h], ag_f2.at[h, d], along(a2, 1))
            f2[h, d, 1] = remote(
                xs.at[h, s(d, 1), :, hi], xs.at[h, s(d, 2), :, hi],
                ag_send.at[h], ag_f2.at[h, d], along(a2, 3))

    both = [(h, k) for h in range(2) for k in range(2)]
    for h, k in both:
        m1[h, k].start()

    w_small, s_small = [], []
    for dz, dx in ORDER[:-1]:
        there = at_ep(dz, dx)
        mine = SLOT[(4 - dz) % 4, (4 - dx) % 4]
        w_small.append(remote(
            w8.at[there[0]], wrow.at[mine], x_send.at[0], x_recv.at[0], there))
        s_small.append(remote(
            sp.at[there[0]], sb.at[0, :, pl.ds(pl.multiple_of(ep * 128, 128), 128)],
            x_send.at[1], x_recv.at[1], there))
    for c in w_small + s_small:
        c.start()
    sb[0, :, pl.ds(pl.multiple_of(ep * 128, 128), 128)] = sp[ep]
    wrow[SLOT[0, 0]] = w8[ep]

    for h, k in both:
        m2[h, 0, k].start()

    s_p, s_m, s_fp, s_fm, s_d, s_l = [], [], [], [], {}, []
    for i, (src, dst) in enumerate([(sg_hbm, sg), (su_hbm, su), (sd_hbm, sd)]):
        s_p.append(remote(src, dst.at[DYI[3]], s_send.at[i], s_recv.at[i, 0], at_y(1)))
        s_m.append(remote(src, dst.at[DYI[1]], s_send.at[i], s_recv.at[i, 1], at_y(3)))
        s_fp.append(remote(
            dst.at[DYI[3], pl.ds(0, 32)], dst.at[DYI[2], pl.ds(0, 32)],
            s_send.at[i], s_frecv.at[i], at_y(1)))
        s_fm.append(remote(
            dst.at[DYI[1], pl.ds(32, 32)], dst.at[DYI[2], pl.ds(32, 32)],
            s_send.at[i], s_frecv.at[i], at_y(3)))
        for dy in DY:
            s_d[i, dy] = remote(
                src if dy == 0 else dst.at[DYI[dy]], dst.at[4 + DYI[dy]],
                s_send.at[i], s_drecv.at[i], partner)
        s_l.append(pltpu.make_async_copy(src, dst.at[0], s_loc.at[i]))

    def silu(v):
        return v / (1.0 + jnp.exp(-v))

    def both_halves(xa, xb, w):
        return lax.dot_general(xa, w[:, :HALF], NT, preferred_element_type=f32) + lax.dot_general(
            xb, w[:, HALF:], NT, preferred_element_type=f32)

    def rows_of(base):
        return (xs[0, pl.ds(base, GROUP)].reshape(ROWS, HALF), xs[1, pl.ds(base, GROUP)].reshape(ROWS, HALF))

    def hidden(base, first, count):
        pattern = wpat[pl.ds(base, GROUP)].reshape(ROWS, 128)
        w2 = jnp.concatenate([pattern, pattern], axis=1)

        def step(c, carry):
            xa, xb = rows_of(base)
            rows = pl.ds(2 * c, 2)
            gate = both_halves(xa, xb, wg[rows].reshape(256, D))
            up = both_halves(xa, xb, wu[rows].reshape(256, D))
            value = (silu(gate) * up * w2).astype(jnp.bfloat16)
            hid[pl.ds(base, GROUP), :, pl.ds(pl.multiple_of(c * 256, 256), 256)] = value.reshape(GROUP, TOK, 256)
            return carry

        lax.fori_loop(first, first + count, step, 0)

    def dense_hidden(base):
        xa, xb = rows_of(base)
        dense = both_halves(xa, xb, wx[...])
        lane = lax.broadcasted_iota(jnp.int32, (ROWS, 128), 1)
        opening = 1.0 / (1.0 + jnp.exp(-dense[:, 64:65]))
        value = jnp.where(lane < 64, silu(dense) * opening, 0.0).astype(jnp.bfloat16)
        hid[pl.ds(base, GROUP), :, pl.ds(1024, 128)] = value.reshape(GROUP, TOK, 128)

    def shared_expert():
        for c in range(2):
            rows = pl.ds(4 * c, 4)
            gate = both_halves(own[0], own[1], sg[rows].reshape(256, D))
            up = both_halves(own[0], own[1], su[rows].reshape(256, D))
            shid[:, pl.ds(256 * c, 256)] = (silu(gate) * up).astype(jnp.bfloat16)

        def step(n, carry):
            cols = pl.ds(pl.multiple_of(n * SUB, SUB), SUB)
            sout[:, cols] = jnp.dot(shid[...], sd[:, :, cols].reshape(512, SUB), preferred_element_type=f32)
            return carry

        lax.fori_loop(0, 4, step, 0)

    def shared_step(part):
        if part == "near":
            for i in range(3):
                s_p[i].wait_recv()
                s_fp[i].start()
                s_d[i, 3].start()
                s_m[i].wait_recv()
                s_fm[i].start()
                s_d[i, 1].start()
        elif part == "far":
            for i in range(3):
                far = (sg, su, sd)[i].at[DYI[2]]
                pltpu.make_async_copy(far, far, s_frecv.at[i]).wait()
                s_d[i, 2].start()
        else:
            for i in range(3):
                s_l[i].wait()
                across = (sg, su, sd)[i].at[pl.ds(4, 4)]
                pltpu.make_async_copy(across, across, s_drecv.at[i]).wait()
            shared_expert()

    def down(base, count):
        def step(n, carry):
            h = n // 2
            cols = pl.ds(pl.multiple_of(n * SUB, SUB), SUB)
            to = pl.ds(pl.multiple_of((n % 2) * SUB, SUB), SUB)
            rows = hid[pl.ds(base, count)].reshape(count * TOK, 1152)
            part = jnp.dot(rows[:, :1024], wd[:, :, cols].reshape(1024, SUB), preferred_element_type=f32)
            part = part + jnp.dot(rows[:, 1024:], wdx[:, cols], preferred_element_type=f32)
            xs[h, pl.ds(base, count), :, to] = part.astype(jnp.bfloat16).reshape(count, TOK, SUB)
            return carry

        lax.fori_loop(0, 4, step, 0)

    def down_early(base):
        def step(n, carry):
            cols = pl.ds(pl.multiple_of(n * SUB, SUB), SUB)
            rows = hid[pl.ds(base, 2)].reshape(2 * TOK, 1152)
            part = jnp.dot(
                rows[:, :768], wd[pl.ds(0, 6), :, cols].reshape(768, SUB), preferred_element_type=f32)
            early[:, cols] = part + jnp.dot(rows[:, 1024:], wdx[:, cols], preferred_element_type=f32)
            return carry

        lax.fori_loop(0, 4, step, 0)

    def down_late(base):
        def step(n, carry):
            h = n // 2
            cols = pl.ds(pl.multiple_of(n * SUB, SUB), SUB)
            to = pl.ds(pl.multiple_of((n % 2) * SUB, SUB), SUB)
            rows = hid[pl.ds(base, 2)].reshape(2 * TOK, 1152)
            part = early[:, cols] + jnp.dot(
                rows[:, 768:1024], wd[pl.ds(6, 2), :, cols].reshape(256, SUB), preferred_element_type=f32)
            xs[h, pl.ds(base, 2), :, to] = part.astype(jnp.bfloat16).reshape(2, TOK, SUB)
            return carry

        lax.fori_loop(0, 4, step, 0)

    for h, k in both:
        m1[h, k].wait_recv()
        f1[h, k].start()
    for h in range(2):
        for d in (3, 1):
            for k in range(2):
                m2[h, d, k].start()

    def weights_on(i):
        w_p[i].wait_recv()
        w_fp[i].start()
        w_d[i, 3].start()
        w_m[i].wait_recv()
        w_fm[i].start()
        w_d[i, 1].start()

    def far_rows(d):
        for h in range(2):
            here = xs.at[h, src_slot(h, d, 2)]
            pltpu.make_async_copy(here, here, ag_f2.at[h, d]).wait()

    def weights_far(i):
        far = (wg, wu, wd)[i].at[2 * DYI[2]]
        pltpu.make_async_copy(far, far, w_frecv.at[i]).wait()
        w_d[i, 2].start()

    weights_on(0)

    pltpu.make_async_copy(wrow.at[pl.ds(0, 15)], wrow.at[pl.ds(0, 15)], x_recv.at[0]).wait()
    columns = jnp.transpose(wrow[...].reshape(128, 128))
    low_lane = lax.broadcasted_iota(jnp.int32, (128, 128), 1) < 64
    for i in range(16):
        first, last, c = columns, columns[:TOK - 128], 8 * i
        wpat[i, pl.ds(0, 128)] = jnp.where(low_lane, first[:, c:c + 1], first[:, c + 2:c + 3])
        wpat[i, pl.ds(128, TOK - 128)] = jnp.where(
            low_lane[:TOK - 128], last[:, c + 1:c + 2], last[:, c + 3:c + 4])

    for h, k in both:
        m2[h, 0, k].wait_recv()
        f2[h, 0, k].start()
    for i in range(2):
        w_l[i].wait()
        w_d[i, 0].wait_recv()
    hidden(GROUPS[0], 0, 1)
    for h, k in both:
        f1[h, k].wait_recv()
    for h in range(2):
        for k in range(2):
            m2[h, 2, k].start()
    pltpu.make_async_copy(
        sb.at[0, :, pl.ds(0, 1920)], sb.at[0, :, pl.ds(0, 1920)], x_recv.at[1]).wait()
    sb_cross = remote(sb.at[0], sb.at[1], sb_dsend, sb_drecv, partner)
    sb_cross.start()
    weights_on(1)
    for i in range(2):
        late_p[i].start()
        late_m[i].start()
    for h, k in both:
        m2[h, 3, k].wait_recv()
        f2[h, 3, k].start()
    for i in range(2):
        w_d[i, 1].wait_recv()
        w_d[i, 3].wait_recv()
    hidden(GROUPS[0], 1, 2)

    sb_cross.wait_recv()
    wx[pl.ds(0, 64), :] = sb[core]
    wdx[pl.ds(0, 64), :] = sb[1 - core]
    dense_hidden(GROUPS[0])
    for h, k in both:
        m2[h, 1, k].wait_recv()
        f2[h, 1, k].start()
    weights_far(0)
    hidden(GROUPS[1], 0, 3)
    weights_far(1)
    far_rows(0)
    for i in range(2):
        w_d[i, 2].wait_recv()
    hidden(GROUPS[0], 3, 1)
    hidden(GROUPS[1], 3, 1)
    late_p[0].wait_recv()
    w_fp[2].start()
    late_m[0].wait_recv()
    w_fm[2].start()
    for i in range(3):
        s_p[i].start()
        s_m[i].start()
    for i in range(3):
        s_d[i, 0].start()
        s_l[i].start()
    for h, k in both:
        m2[h, 2, k].wait_recv()
        f2[h, 2, k].start()
    dense_hidden(GROUPS[1])
    far_rows(3)
    hidden(GROUPS[2], 0, 2)
    late_p[1].wait_recv()
    w_d[2, 3].start()
    late_m[1].wait_recv()
    w_d[2, 1].start()
    hidden(GROUPS[2], 2, 2)
    dense_hidden(GROUPS[2])
    weights_far(2)
    w_l[2].wait()
    for dy in (0, 1, 3):
        w_d[2, dy].wait_recv()
    down_early(PARTS["g2b"][0])
    far_rows(1)
    far_rows(2)
    for h in range(2):
        pltpu.make_async_copy(xs.at[h, pl.ds(0, 15)], xs.at[h, pl.ds(0, 15)], ag_send.at[h]).wait()
    w_d[2, 2].wait_recv()

    rs_axes = [("z", "x"), ("x", "z")]

    def dst_slot(h, d1, q):
        return SLOT[(d1, q) if h == 0 else (q, d1)]

    r1, s1, e1, r2, s2, e2 = {}, {}, {}, {}, {}, {}
    halves = [lo, hi]
    for h in range(2):
        b1, b2 = rs_axes[h]
        t = functools.partial(dst_slot, h)
        for k in range(2):
            sum_cols, own_cols = halves[k], halves[1 - k]
            near, step = (1, 3)[k], (1, 3)[k]
            for q in range(4):
                to = along(b1, step)
                r1[h, q, k] = remote(
                    xs.at[h, t(2, q), :, sum_cols], rl.at[h, q, k], rs_send.at[h], rl_sem.at[h, q, k], to)
                s1[h, q, k] = remote(
                    xs.at[h, t(near, q), :, sum_cols], rf.at[h, q, k, :, sum_cols],
                    rs_send.at[h], rf_sem.at[h, q], to)
                e1[h, q, k] = remote(
                    xs.at[h, t(near, q), :, own_cols], rf.at[h, q, k, :, own_cols],
                    rs_send.at[h], rf_sem.at[h, q], to)
            to = along(b2, step)
            for p in range(2):
                cols = pl.ds(SUB * k + QUARTER * p, QUARTER)
                r2[h, p, k] = remote(
                    xs.at[h, t(0, 2), :, cols], rl2.at[h, k, :, pl.ds(QUARTER * p, QUARTER)],
                    rs_send.at[h], rl2_sem.at[h, p, k], to)
                s2[h, p, k] = remote(
                    xs.at[h, t(0, near), :, cols], rf2.at[h, k, :, cols],
                    rs_send.at[h], rf2_sem.at[h, k, p], to)
            e2[h, k] = remote(
                xs.at[h, t(0, near), :, own_cols], rf2.at[h, k, :, own_cols],
                rs_send.at[h], rf2_sem.at[h, k, 2], to)

    def add(slot, h, cols, *more):
        total = xs[h, slot, :, cols].astype(f32)
        for m in more:
            total = total + m.astype(f32)
        xs[h, slot, :, cols] = total.astype(jnp.bfloat16)

    for op in SUM_ORDER:
        name = op[0]
        if name == "C":
            if op[1] == "g2b":
                down_late(PARTS["g2b"][0])
            else:
                down(*PARTS[op[1]])
            continue
        if name == "U":
            hidden(GROUPS[3], op[1], op[2])
            if op[1] + op[2] == 4:
                dense_hidden(GROUPS[3])
            continue
        if name == "S":
            shared_step(op[1])
            continue
        _, h, q, k = op
        near = (1, 3)[k]
        if name == "relay":
            r1[h, q, k].start()
        elif name == "free":
            e1[h, q, k].start()
        elif name == "pass":
            r1[h, q, k].wait_recv()
            add(dst_slot(h, near, q), h, halves[k], rl[h, q, k])
            s1[h, q, k].start()
        elif name == "collect":
            pltpu.make_async_copy(rf.at[h, q], rf.at[h, q], rf_sem.at[h, q]).wait()
            add(dst_slot(h, 0, q), h, pl.ds(0, HALF), rf[h, q, 0], rf[h, q, 1])
        elif name == "relay2":
            r2[h, q, k].start()
        elif name == "free2":
            e2[h, k].start()
        elif name == "pass2":
            r2[h, q, k].wait_recv()
            add(
                dst_slot(h, 0, near), h, pl.ds(SUB * k + QUARTER * q, QUARTER),
                rl2[h, k, :, pl.ds(QUARTER * q, QUARTER)])
            s2[h, q, k].start()
        else:
            for i in range(2):
                e2[h, i].wait_recv()
                s2[h, 0, i].wait_recv()
                s2[h, 1, i].wait_recv()
            total = xs[h, SLOT[0, 0]].astype(f32) + rf2[h, 0].astype(f32) + rf2[h, 1].astype(f32)
            total = total + sout[:, pl.ds(h * HALF, HALF)]
            out_ref[:, pl.ds(h * HALF, HALF)] = total.astype(jnp.bfloat16)

    for h in range(2):
        pltpu.make_async_copy(xs.at[h, pl.ds(0, 15)], xs.at[h, pl.ds(0, 15)], rs_send.at[h]).wait()
    for sent, sem in ((wg, w_send.at[0]), (wu, w_send.at[1]), (wd, w_send.at[2])):
        pltpu.make_async_copy(sent.at[pl.ds(0, 7)], sent.at[pl.ds(0, 7)], sem).wait()
    for i, sent in enumerate((sg, su, sd)):
        pltpu.make_async_copy(sent.at[pl.ds(0, 7)], sent.at[pl.ds(0, 7)], s_send.at[i]).wait()
    pltpu.make_async_copy(wrow.at[pl.ds(0, 15)], wrow.at[pl.ds(0, 15)], x_send.at[0]).wait()
    pltpu.make_async_copy(
        sb.at[0, :, pl.ds(0, 1920)], sb.at[0, :, pl.ds(0, 1920)], x_send.at[1]).wait()
    sb_cross.wait_send()


def body(
    tokens, norm_gain, expert_ids, route_weights, expert_gate, expert_up, expert_down,
    shared_gate, shared_up, shared_down, side_in, side_out, side_gate,
):
    bf16, f32 = jnp.bfloat16, jnp.float32
    dma, vmem = pltpu.SemaphoreType.DMA, pltpu.VMEM
    in_vmem = pl.BlockSpec(memory_space=pltpu.VMEM)
    in_any = pl.BlockSpec(memory_space=pl.ANY)
    return pl.pallas_call(
        kernel,
        out_shape=pltpu.VMEM((TOK, D), bf16),
        in_specs=[in_any] * 13,
        out_specs=in_vmem,
        scratch_shapes=[
            vmem((TOK, D), bf16),
            vmem((1, D), f32),
            vmem((8, TOK), jnp.int32),
            vmem((8, TOK), f32),
            vmem((128, 1024), bf16),
            vmem((16, 128), bf16),
            dma((6,)),
            vmem((2, 16, TOK, HALF), bf16),
            vmem((2, TOK, HALF), bf16),
            vmem((8, 128, D), bf16),
            vmem((8, 128, D), bf16),
            vmem((8, 128, D), bf16),
            vmem((128, D), bf16),
            vmem((128, D), bf16),
            vmem((2, 64, D), bf16),
            vmem((16, 64, 128), bf16),
            vmem((8, 64, D), bf16),
            vmem((8, 64, D), bf16),
            vmem((8, 64, D), bf16),
            vmem((TOK, 512), bf16),
            vmem((TOK, D), f32),
            vmem((16, TOK, 1152), bf16),
            vmem((2 * TOK, D), f32),
            vmem((2, 4, 2, TOK, SUB), bf16),
            vmem((2, 4, 2, TOK, HALF), bf16),
            vmem((2, 2, TOK, SUB), bf16),
            vmem((2, 2, TOK, HALF), bf16),
            vmem((16, 8, 128), f32),
            vmem((16, 8, 128), f32),
            vmem((16, TOK, 128), f32),
            dma((2,)), dma((2, 2)), dma((2, 2)), dma((2, 4, 2)), dma((2, 4)),
            dma((3,)), dma((2, 2)), dma((3,)), dma((3, 4)), dma((3,)), dma((2, 2)),
            dma((2,)), dma((2,)), dma(()), dma(()),
            dma((3,)), dma((3, 2)), dma((3,)), dma((3,)), dma((3,)),
            dma((2,)), dma((2, 4, 2)), dma((2, 4)), dma((2, 2, 2)), dma((2, 2, 3)),
        ],
        compiler_params=pltpu.CompilerParams(
            collective_id=0, has_side_effects=True, vmem_limit_bytes=60 * 1024 * 1024),
        name="routed_layer",
    )(
        tokens, norm_gain.reshape(1, D), expert_ids.T, route_weights.T,
        expert_gate.reshape(128, D), expert_up.reshape(128, D), expert_down.reshape(128, D),
        shared_gate, shared_up, shared_down, side_in, side_out, side_gate.reshape(16, 128),
    )


def solution(mesh):
    placed = (
        P(("ep", "tp"), None),
        P(),
        P(("ep", "tp"), None),
        P(("ep", "tp"), None),
        P("ep", "tp", None),
        P("ep", "tp", None),
        P("ep", "tp", None),
        P("tp", None),
        P("tp", None),
        P("tp", None),
        P("ep", None),
        P("ep", None),
        P(),
    )
    return jax.shard_map(
        body, mesh=mesh, in_specs=placed, out_specs=P(("ep", "tp"), None), check_vma=False
    )
```
